32 devices in a mesh: sp: 16 (over z, y, x), tp: 2 (over core).
Axes of the slice: x: 2, y: 2, z: 4, core: 2. Of those that a mesh axis runs over, the one named last changes fastest.
Arguments:
- projected_queries: bfloat16 [8192, 1024], P('sp', 'tp'), may hold values from -6 to 6
- projected_keys: bfloat16 [8192, 1024], P('sp', 'tp'), may hold values from -6 to 6
- projected_values: bfloat16 [8192, 1024], P('sp', 'tp'), may hold values from -6 to 6
- output_gate_values: bfloat16 [8192, 1024], P('sp', 'tp'), may hold values from -6 to 6
- write_strength_logits: bfloat16 [8192, 8], P('sp', 'tp'), may hold values from -6.5 to 3
- decay_input_logits: bfloat16 [8192, 8], P('sp', 'tp'), may hold values from -5 to 5
- head_rate_logarithm: float32 [8], P('tp'), may hold values from -8 to 2.3
- extra_log_decay: float32 [8192, 8], P('sp', 'tp'), may hold values from -0.7 to 0
- per_head_norm_gain: float32 [128], replicated, may hold values from 0.1 to 1.9
- output_matrix: bfloat16 [1024, 2048], replicated, may hold values from -0.1875 to 0.1875
- residual: bfloat16 [8192, 2048], P(('sp', 'tp')), may hold values from -6 to 6
- mixture_norm_gain: float32 [2048], replicated, may hold values from 0.1 to 1.9
- selected_expert_index: int32 [8192, 4], P(('sp', 'tp')), may hold values from 0 to 31, all different within a row; in each aligned block of 256 rows (0 to 255, 256 to 511, ...) at most 48 rows name the same one
- routing_weight: float32 [8192, 4], P(('sp', 'tp')), may hold values from 0.1 to 0.9
- routed_gate_weight: bfloat16 [32, 2048, 512], P(('sp', 'tp')), may hold values from -0.125 to 0.125
- routed_up_weight: bfloat16 [32, 2048, 512], P(('sp', 'tp')), may hold values from -0.125 to 0.125
- routed_down_weight: bfloat16 [32, 512, 2048], P(('sp', 'tp')), may hold values from -0.25 to 0.25
- common_gate_weight: bfloat16 [2048, 512], replicated, may hold values from -0.125 to 0.125
- common_up_weight: bfloat16 [2048, 512], replicated, may hold values from -0.125 to 0.125
- common_down_weight: bfloat16 [512, 2048], replicated, may hold values from -0.25 to 0.25
Outputs:
- block_out: bfloat16 [8192, 2048], P(('sp', 'tp'))
The draws below stay inside these ranges and needn't reach their ends.
Inputs may be any that keep to these rules, and one draw needn't show every extreme that they name: `selected_expert_index`: each row names 4 different experts. Among the rows that one device holds, no expert is named more than 48 times.
All inputs are finite; a program needn't handle non-finite values.
Results may differ from the reference program's by a relative error of at most 0.008.
Values may be sent and summed in bfloat16 or wider, within the bound.
A program may use at most 192 MiB of HBM per device.

```python
import math
import jax
import jax.numpy as jnp
import numpy as np
from jax import lax

D = 2048
HEADS = 8
HD = 128
EFF = 512
SFF = 512
TOP_K = 4
SPAN = 64
TOK_DEV = 512
TOKENS = 8192
EXPERTS = 32
CAP = 48
N_SP = 16
N_TP = 2


def head_order(key):
    return jax.random.permutation(jax.random.fold_in(key, 11), HEADS)


def draw_head_rate_logarithm(key, part):
    order = head_order(key)
    jitter = jax.random.uniform(jax.random.fold_in(key, 12), (HEADS,), jnp.float32, -0.4, 0.4)
    fast = order < HEADS // 2
    slow_level = math.log(244.0 / TOKENS)
    return jnp.where(fast, 1.8, slow_level).astype(jnp.float32) + jitter


def draw_write_strength_logits(key, part):
    order = head_order(key)
    fast = order < HEADS // 2
    blocks = TOKENS // TOK_DEV
    level = jax.random.uniform(jax.random.fold_in(key, 41), (blocks, 1, HEADS), jnp.float32, -5.5, -4.5)
    jiggle = jax.random.uniform(jax.random.fold_in(key, 42), (blocks, TOK_DEV, HEADS), jnp.float32, -1.0, 1.0)
    wide = jax.random.uniform(jax.random.fold_in(key, 43), (blocks, TOK_DEV, HEADS), jnp.float32, -3.0, 3.0)
    picked = jnp.where(fast[None, None, :], wide, level + jiggle)
    return picked.reshape(TOKENS, HEADS).astype(jnp.bfloat16)


def draw_decay_input_logits(key, part):
    shifts = jax.random.uniform(jax.random.fold_in(key, 21), (TOKENS // TOK_DEV, 1, HEADS), jnp.float32, -0.8, 0.8)
    noise = jnp.clip(jax.random.normal(jax.random.fold_in(key, 22), (TOKENS // TOK_DEV, TOK_DEV, HEADS), jnp.float32), -3.5, 3.5)
    return (noise + shifts).reshape(TOKENS, HEADS).astype(jnp.bfloat16)


def draw_extra_log_decay(key, part):
    chance = jax.random.uniform(jax.random.fold_in(key, 31), (TOKENS, HEADS), jnp.float32)
    depth = jax.random.uniform(jax.random.fold_in(key, 32), (TOKENS, HEADS), jnp.float32, 0.22, 0.69)
    return jnp.where(chance < 6.0 / TOKENS, -depth, 0.0).astype(jnp.float32)


def steps_of(stream_key, dims, shards, low, largest):
    def one(dim, blocks):
        draws = jax.random.uniform(jax.random.fold_in(jax.random.fold_in(stream_key, 6), dim), (blocks,), jnp.float32, low / len(shards), largest / len(shards))
        return jnp.repeat(jnp.exp(draws), dims[dim] // blocks).reshape((-1,) + (1,) * (len(dims) - dim - 1))

    level = one(*shards[0])
    for cut in shards[1:]:
        level = level * one(*cut)
    return level


def routed_block(own_key, own, number, rows, count, top, most, slope):
    sequence = jax.random.permutation(own_key, count)
    crowded, ordinary = shares(count, rows * top, most, slope, True), shares(count, rows * top, most, slope, False)
    places = jnp.arange(count)

    def named(lengths, rotation):
        used = int((lengths > 0).sum())
        fixed = max(1, used // 4)
        shifted = fixed + (places - fixed + rotation * (used - fixed)) % max(1, count - fixed)
        return jnp.zeros((count,), jnp.int32).at[sequence[jnp.where(places < fixed, places, shifted)]].set(jnp.asarray(lengths, jnp.int32))

    lengths = jnp.where(number % 4 == 0, named(crowded, number // 4), named(ordinary, number - number // 4 - 1))
    mixed = jax.random.permutation(jax.random.fold_in(own, 3), count)
    giver, taker = mixed[0:count // 2 * 2:2], mixed[1:count // 2 * 2:2]
    slack = jnp.minimum(lengths[giver] - 1, most - lengths[taker]) // 2
    slack = jnp.where((giver == sequence[0]) | (taker == sequence[0]) | (lengths[taker] == 0), 0, jnp.maximum(slack, 0))
    shifted = jax.random.randint(jax.random.fold_in(own, 4), (count // 2,), 0, 1 << 20) % (slack + 1)
    lengths = lengths.at[giver].add(-shifted).at[taker].add(shifted)
    items = jnp.searchsorted(jnp.cumsum(lengths), jnp.arange(rows * top), side="right").astype(jnp.int32)
    grid = items.reshape(top, rows).T
    grid = grid[jax.random.permutation(jax.random.fold_in(own, 1), rows)]
    rotation = jax.random.randint(jax.random.fold_in(own, 2), (rows, 1), 0, top)
    return jnp.take_along_axis(grid, (jnp.arange(top)[None, :] + rotation) % top, axis=1)


def shares(number_of, total, most, lean, full):
    loads = [(1 << 20) // math.isqrt(grade ** lean) + 1 for grade in range(1, number_of + 1)]
    largest = most if full else min(most, max(-(-total // number_of), total * loads[0] // sum(loads)))
    least = 1 if total - largest >= number_of - 1 else 0
    holding, surplus = [largest] + [least] * (number_of - 1), total - largest - least * (number_of - 1)
    while surplus > 0:
        free = [i for i in range(1, number_of) if holding[i] < largest] or [i for i in range(1, number_of) if holding[i] < most]
        whole, remaining = sum([loads[i] for i in free]), surplus
        for i in free:
            addition = min(most - holding[i], max(1, remaining * loads[i] // whole), surplus)
            holding[i] = holding[i] + addition
            surplus = surplus - addition
    return np.array(holding)


def gaussian(stream_key, shape, scale, most, pieces=(), kind=jnp.bfloat16):
    values = jax.random.normal(stream_key, shape, jnp.float32) * scale
    if len(pieces) > 0:
        values = steps_of(stream_key, shape, pieces, -0.22, 0.18) * values
    return jnp.clip(values, min=-most, max=most).astype(kind)


def setup_inputs(seed: int = 0) -> dict:
    splits = jax.random.split(jax.random.key(seed), 21)
    projected_queries = gaussian(splits[0], (TOKENS, HEADS * HD), 1.0, 6.0, ((0, 16), (1, 2)))
    projected_keys = gaussian(splits[1], (TOKENS, HEADS * HD), 1.0, 6.0, ((0, 16), (1, 2)))
    projected_values = gaussian(splits[2], (TOKENS, HEADS * HD), 1.0, 6.0, ((0, 16), (1, 2)))
    output_gate_values = gaussian(splits[3], (TOKENS, HEADS * HD), 1.0, 6.0, ((0, 16), (1, 2)))
    write_strength_logits = draw_write_strength_logits(jax.random.fold_in(splits[20], 71), 0)
    decay_input_logits = draw_decay_input_logits(jax.random.fold_in(splits[20], 71), 0)
    head_rate_logarithm = draw_head_rate_logarithm(jax.random.fold_in(splits[20], 71), 0)
    extra_log_decay = draw_extra_log_decay(jax.random.fold_in(splits[20], 71), 0)
    per_head_norm_gain = jnp.clip(1.0 + 0.18 * jax.random.normal(splits[8], (HD,), jnp.float32), 0.1, 1.9)
    output_matrix = gaussian(splits[9], (HEADS * HD, D), (HEADS * HD) ** -0.5, 0.1875)
    residual = gaussian(splits[10], (TOKENS, D), 1.0, 6.0, ((0, 32),))
    mixture_norm_gain = jnp.clip(1.0 + 0.18 * jax.random.normal(splits[11], (D,), jnp.float32), 0.1, 1.9)
    selected_expert_index_keys = jax.random.split(jax.random.fold_in(splits[12], 1), TOKENS // (TOK_DEV // N_TP))
    selected_expert_index_turns = jax.random.permutation(jax.random.fold_in(splits[12], 3), TOKENS // (TOK_DEV // N_TP))
    selected_expert_index = jax.vmap(lambda own, number: routed_block(jax.random.fold_in(splits[12], 2), own, number, TOK_DEV // N_TP, EXPERTS, TOP_K, CAP, 1))(selected_expert_index_keys, selected_expert_index_turns).reshape((TOKENS, TOP_K))
    routing_weight = jnp.clip(0.1 + 0.79999997 * jax.random.uniform(splits[13], (TOKENS, TOP_K), jnp.float32) ** steps_of(splits[13], (TOKENS, TOP_K), ((0, 32),), -0.2, 0.2), 0.1, 0.9)
    routed_gate_weight = gaussian(splits[14], (EXPERTS, D, EFF), D ** -0.5, 0.125, ((0, 32),))
    routed_up_weight = gaussian(splits[15], (EXPERTS, D, EFF), D ** -0.5, 0.125, ((0, 32),))
    routed_down_weight = gaussian(splits[16], (EXPERTS, EFF, D), EFF ** -0.5, 0.25, ((0, 32),))
    common_gate_weight = gaussian(splits[17], (D, SFF), D ** -0.5, 0.125)
    common_up_weight = gaussian(splits[18], (D, SFF), D ** -0.5, 0.125)
    common_down_weight = gaussian(splits[19], (SFF, D), SFF ** -0.5, 0.25)
    return dict(projected_queries=projected_queries, projected_keys=projected_keys, projected_values=projected_values, output_gate_values=output_gate_values, write_strength_logits=write_strength_logits, decay_input_logits=decay_input_logits, head_rate_logarithm=head_rate_logarithm, extra_log_decay=extra_log_decay, per_head_norm_gain=per_head_norm_gain, output_matrix=output_matrix, residual=residual, mixture_norm_gain=mixture_norm_gain, selected_expert_index=selected_expert_index, routing_weight=routing_weight, routed_gate_weight=routed_gate_weight, routed_up_weight=routed_up_weight, routed_down_weight=routed_down_weight, common_gate_weight=common_gate_weight, common_up_weight=common_up_weight, common_down_weight=common_down_weight)


EPS = 1e-06
HIGH = lax.Precision.HIGHEST

def unit_heads(raw, heads):
    active = jax.nn.silu(raw.astype(jnp.float32)).reshape(raw.shape[0], heads, -1)
    return active * lax.rsqrt(lax.optimization_barrier(jnp.sum(active * active, axis=-1, keepdims=True)) + EPS)

def prepare_inputs(projected_queries, projected_keys, projected_values, write_strength_logits, decay_input_logits, head_rate_logarithm, extra_log_decay):
    heads = head_rate_logarithm.shape[0]
    queries = unit_heads(projected_queries, heads)
    keys = unit_heads(projected_keys, heads)
    values = jax.nn.silu(projected_values.astype(jnp.float32)).reshape(projected_values.shape[0], heads, -1)
    beta = jax.nn.sigmoid(write_strength_logits.astype(jnp.float32))
    decay_logarithm = extra_log_decay - jnp.exp(head_rate_logarithm)[None, :] * jax.nn.softplus(decay_input_logits.astype(jnp.float32) - 6.0)
    return (queries, keys, values, beta, decay_logarithm)

def block_terms(queries, keys, values, beta, decay_logarithm):
    length, heads, width = queries.shape
    number = length // SPAN

    def split(array):
        return jnp.moveaxis(array.reshape(number, SPAN, heads, -1), 2, 0)
    q_blocks = split(queries)
    k_blocks = split(keys)
    v_blocks = split(values)
    b_blocks = split(beta[..., None])[..., 0]
    g_cumul = jnp.cumsum(split(decay_logarithm[..., None])[..., 0], axis=-1)
    place = jnp.arange(SPAN)
    causal = place[:, None] >= place[None, :]
    strict = place[:, None] > place[None, :]
    spread = jnp.where(causal, g_cumul[..., :, None] - g_cumul[..., None, :], 0.0)
    decay = jnp.where(causal, jnp.exp(spread), 0.0)
    k_beta = k_blocks * b_blocks[..., None]
    inner = jnp.einsum('hncd,hnsd->hncs', k_beta, k_blocks, precision=HIGH)
    lower = jnp.where(strict, inner * decay, 0.0) + jnp.eye(SPAN, dtype=jnp.float32)
    right = jnp.concatenate([v_blocks * b_blocks[..., None], k_beta * jnp.exp(g_cumul)[..., None]], axis=-1)
    solved = jax.scipy.linalg.solve_triangular(lower, right, lower=True, unit_diagonal=True)
    u_part = solved[..., :width]
    w_part = solved[..., width:]
    scores = jnp.einsum('hncd,hnsd->hncs', q_blocks, k_blocks, precision=HIGH) * decay
    q_decayed = q_blocks * jnp.exp(g_cumul)[..., None]
    log_last = g_cumul[..., -1]
    k_decayed = k_blocks * jnp.exp(log_last[..., None] - g_cumul)[..., None]
    return (q_decayed, scores, u_part, w_part, k_decayed, log_last)

def run_blocks(terms, start):

    def advance(state, items):
        q_one, s_one, u_one, w_one, k_one, log_one = items
        fresh = u_one - jnp.einsum('hcd,hde->hce', w_one, state, precision=HIGH)
        result = jnp.einsum('hcd,hde->hce', q_one, state, precision=HIGH)
        result = result + jnp.einsum('hcs,hse->hce', s_one, fresh, precision=HIGH)
        state = state * jnp.exp(log_one)[:, None, None] + jnp.einsum('hcd,hce->hde', k_one, fresh, precision=HIGH)
        return (state, result)
    items = tuple((jnp.moveaxis(array, 1, 0) for array in terms))
    _, results = lax.scan(advance, start, items)
    number, heads, span, width = results.shape
    return results.transpose(0, 2, 1, 3).reshape(number * span, heads, width)

def finish(head_mix, output_gate_values, per_head_norm_gain):
    length, heads, width = head_mix.shape
    scaled = head_mix * lax.rsqrt(lax.optimization_barrier(jnp.mean(head_mix * head_mix, axis=-1, keepdims=True)) + EPS)
    gated = scaled * per_head_norm_gain * jax.nn.silu(output_gate_values.astype(jnp.float32).reshape(length, heads, width))
    return gated.reshape(length, heads * width).astype(jnp.bfloat16)

def normalize(stream, gain):
    wide = stream.astype(jnp.float32)
    return (wide * lax.rsqrt(lax.optimization_barrier(jnp.mean(wide * wide, axis=-1, keepdims=True)) + EPS) * gain).astype(jnp.bfloat16)

def feed_forward(rows, w_gate, w_up, w_down):
    hidden = jax.nn.silu(jnp.dot(rows.astype(jnp.float32), w_gate.astype(jnp.float32), preferred_element_type=jnp.float32))
    hidden = (hidden * jnp.dot(rows.astype(jnp.float32), w_up.astype(jnp.float32), preferred_element_type=jnp.float32)).astype(jnp.bfloat16)
    return jnp.dot(hidden.astype(jnp.float32), w_down.astype(jnp.float32), preferred_element_type=jnp.float32)

def routed_sum(normed, selected_expert_index, routing_weight, routed_gate_weight, routed_up_weight, routed_down_weight):
    length = normed.shape[0]
    room = N_SP * N_TP * CAP
    flat_ids = selected_expert_index.reshape(-1)
    flat_rows = (jnp.arange(flat_ids.shape[0]) // TOP_K).astype(jnp.int32)
    flat_weight = routing_weight.reshape(-1)

    def one_expert(total, items):
        w_gate, w_up, w_down, expert = items
        chosen = flat_ids == expert
        slot = (jnp.cumsum(chosen.astype(jnp.int32)) - 1).astype(jnp.int32)
        target = jnp.where(chosen, slot, room).astype(jnp.int32)
        source = jnp.zeros((room,), jnp.int32).at[target].set(flat_rows, mode='drop')
        weight = jnp.zeros((room,), jnp.float32).at[target].set(flat_weight, mode='drop')
        result = feed_forward(normed[source], w_gate, w_up, w_down).astype(jnp.bfloat16)
        return (total.at[source].add(result.astype(jnp.float32) * weight[:, None]), None)
    experts_all = jnp.arange(EXPERTS).astype(jnp.int32)
    total, _ = lax.scan(one_expert, jnp.zeros((length, D), jnp.float32), (routed_gate_weight, routed_up_weight, routed_down_weight, experts_all))
    return total

def reference(projected_queries, projected_keys, projected_values, output_gate_values, write_strength_logits, decay_input_logits, head_rate_logarithm, extra_log_decay, per_head_norm_gain, output_matrix, residual, mixture_norm_gain, selected_expert_index, routing_weight, routed_gate_weight, routed_up_weight, routed_down_weight, common_gate_weight, common_up_weight, common_down_weight):
    prepared_inputs = prepare_inputs(projected_queries, projected_keys, projected_values, write_strength_logits, decay_input_logits, head_rate_logarithm, extra_log_decay)
    terms = block_terms(*prepared_inputs)
    start = jnp.zeros((HEADS, HD, HD), jnp.float32)
    heads_out = finish(run_blocks(terms, start), output_gate_values, per_head_norm_gain)
    attended = residual.astype(jnp.float32) + jnp.dot(heads_out.astype(jnp.float32), output_matrix.astype(jnp.float32), preferred_element_type=jnp.float32)
    attended = attended.astype(jnp.bfloat16)
    normed = normalize(attended, mixture_norm_gain)
    shared = feed_forward(normed, common_gate_weight, common_up_weight, common_down_weight)
    routed = routed_sum(normed, selected_expert_index, routing_weight, routed_gate_weight, routed_up_weight, routed_down_weight)
    return (attended.astype(jnp.float32) + shared + routed).astype(jnp.bfloat16)
```

```python
import functools

import jax
import jax.numpy as jnp
from jax import lax
from jax.experimental import pallas as pl
from jax.experimental.pallas import tpu as pltpu
from jax.sharding import PartitionSpec as P

TOP_K = 4
SPAN = 64


EPS = 1e-06
HIGH = lax.Precision.HIGHEST


def exchange_kernel(axes, sizes, x_ref, o_ref, held, send_sem, recv_sem, local_sem):
    count = 1
    me = 0
    for axis, size in zip(axes, sizes):
        count *= size
        me = me * size + lax.axis_index(axis)

    def device(index):
        found = {}
        for axis, size in reversed(list(zip(axes, sizes))):
            found[axis] = lax.rem(index, size)
            index = index // size
        return found

    barrier = pltpu.get_barrier_semaphore()
    for step in range(1, count):
        pl.semaphore_signal(
            barrier,
            inc=1,
            device_id=device(lax.rem(me + step, count)),
            device_id_type=pl.DeviceIdType.MESH,
        )
    pl.semaphore_wait(barrier, count - 1)
    copies = []
    for step in range(1, count):
        peer = lax.rem(me + step, count)
        copy = pltpu.make_async_remote_copy(
            src_ref=x_ref.at[peer],
            dst_ref=o_ref.at[me],
            send_sem=send_sem.at[step],
            recv_sem=recv_sem.at[step],
            device_id=device(peer),
            device_id_type=pl.DeviceIdType.MESH,
        )
        copy.start()
        copies.append(copy)
    into = pltpu.make_async_copy(x_ref.at[me], held, local_sem)
    into.start()
    into.wait()
    out = pltpu.make_async_copy(held, o_ref.at[me], local_sem)
    out.start()
    out.wait()
    for copy in copies:
        copy.wait()


def exchange(value, axes, identity):
    sizes = tuple(lax.axis_size(axis) for axis in axes)
    count = value.shape[0]
    return pl.pallas_call(
        functools.partial(exchange_kernel, axes, sizes),
        out_shape=jax.ShapeDtypeStruct(value.shape, value.dtype),
        in_specs=[pl.BlockSpec(memory_space=pl.ANY)],
        out_specs=pl.BlockSpec(memory_space=pl.ANY),
        scratch_shapes=[
            pltpu.VMEM(value.shape[1:], value.dtype),
            pltpu.SemaphoreType.DMA((count,)),
            pltpu.SemaphoreType.DMA((count,)),
            pltpu.SemaphoreType.DMA,
        ],
        compiler_params=pltpu.CompilerParams(collective_id=identity, has_side_effects=True),
    )(value)


def shift_join(stacked, step, width):
    later = stacked[:, step:]
    joined = jnp.einsum(
        "hned,hndf->hnef", stacked[:, :-step], later[:, :, :width], precision=HIGH
    )
    joined = jnp.concatenate(
        [joined[:, :, :width], joined[:, :, width:] + later[:, :, width:]], axis=2
    )
    return jnp.concatenate([stacked[:, :step], joined], axis=1)


def inclusive(stacked, width):
    step = 1
    while step < stacked.shape[1]:
        stacked = shift_join(stacked, step, width)
        step *= 2
    return stacked


def starts_of(total):
    heads, _, width = total.shape
    count = lax.axis_size("sp")
    parts = count // heads
    mapping = jnp.repeat(total[:, :width], parts, axis=0)
    carried = total[:, width:].reshape(count, width // parts, width)
    arrived = exchange(jnp.concatenate([mapping, carried], axis=1), ("sp",), 0)
    joined = inclusive(arrived[None], width)[0, :, width:]
    before = jnp.concatenate([jnp.zeros_like(joined[:1]), joined[:-1]], axis=0)
    return exchange(before, ("sp",), 1).reshape(heads, width, width)


def invert_kernel(n_ref, x_ref):
    span = n_ref.shape[-1]
    row = lax.broadcasted_iota(jnp.int32, (span, span), 0)
    column = lax.broadcasted_iota(jnp.int32, (span, span), 1)
    one = (row == column).astype(jnp.float32)
    strict = [n_ref[i] for i in range(n_ref.shape[0])]
    found = None
    size = 1
    while size < span:
        pair = (row // size) - (column // size)
        mask = ((row // size) % 2 == 1) & (pair == 1)
        below = [jnp.where(mask, part, 0.0) for part in strict]
        if found is None:
            found = [one - part for part in below]
        else:
            inner = [
                jnp.dot(x, part, precision=HIGH, preferred_element_type=jnp.float32)
                for x, part in zip(found, below)
            ]
            found = [
                x - jnp.dot(y, x, precision=HIGH, preferred_element_type=jnp.float32)
                for x, y in zip(found, inner)
            ]
        size *= 2
    for i, x in enumerate(found):
        x_ref[i] = x


def invert_unit_lower(strict):
    number, span, _ = strict.shape
    group = 8 if number % 8 == 0 else 1
    spec = pl.BlockSpec((group, span, span), lambda i: (i, 0, 0))
    return pl.pallas_call(
        invert_kernel,
        grid=(number // group,),
        out_shape=jax.ShapeDtypeStruct(strict.shape, jnp.float32),
        in_specs=[spec],
        out_specs=spec,
    )(strict)


def unit_heads(raw, heads):
    active = jax.nn.silu(raw.astype(jnp.float32)).reshape(raw.shape[0], heads, -1)
    return active * lax.rsqrt(jnp.sum(active * active, axis=-1, keepdims=True) + EPS)


def prepare_inputs(
    projected_queries,
    projected_keys,
    projected_values,
    write_strength_logits,
    decay_input_logits,
    head_rate_logarithm,
    extra_log_decay,
):
    heads = head_rate_logarithm.shape[0]
    queries = unit_heads(projected_queries, heads)
    keys = unit_heads(projected_keys, heads)
    values = jax.nn.silu(projected_values.astype(jnp.float32)).reshape(
        projected_values.shape[0], heads, -1
    )
    beta = jax.nn.sigmoid(write_strength_logits.astype(jnp.float32))
    decay_logarithm = extra_log_decay - jnp.exp(head_rate_logarithm)[None, :] * jax.nn.softplus(
        decay_input_logits.astype(jnp.float32) - 6.0
    )
    return (queries, keys, values, beta, decay_logarithm)


def block_terms(queries, keys, values, beta, decay_logarithm):
    length, heads, width = queries.shape
    number = length // SPAN

    def split(array):
        return jnp.moveaxis(array.reshape(number, SPAN, heads, -1), 2, 0)

    q_blocks = split(queries)
    k_blocks = split(keys)
    v_blocks = split(values)
    b_blocks = split(beta[..., None])[..., 0]
    g_cumul = jnp.cumsum(split(decay_logarithm[..., None])[..., 0], axis=-1)
    place = jnp.arange(SPAN)
    causal = place[:, None] >= place[None, :]
    strict = place[:, None] > place[None, :]
    spread = jnp.where(causal, g_cumul[..., :, None] - g_cumul[..., None, :], 0.0)
    decay = jnp.where(causal, jnp.exp(spread), 0.0)
    k_beta = k_blocks * b_blocks[..., None]
    inner = jnp.einsum("hncd,hnsd->hncs", k_beta, k_blocks, precision=HIGH)
    lower = jnp.where(strict, inner * decay, 0.0)
    inverse = invert_unit_lower(lower.reshape(heads * number, SPAN, SPAN)).reshape(lower.shape)
    right = jnp.concatenate(
        [k_beta * jnp.exp(g_cumul)[..., None], v_blocks * b_blocks[..., None]], axis=-1
    )
    solved = jnp.einsum("hncs,hnsd->hncd", inverse, right, precision=HIGH)
    scores = jnp.einsum("hncd,hnsd->hncs", q_blocks, k_blocks, precision=HIGH) * decay
    q_decayed = q_blocks * jnp.exp(g_cumul)[..., None]
    log_last = g_cumul[..., -1]
    k_decayed = k_blocks * jnp.exp(log_last[..., None] - g_cumul)[..., None]
    return (q_decayed, scores, solved, k_decayed, log_last)


def mix_heads(terms):
    q_decayed, scores, solved, k_decayed, log_last = terms
    heads, number, span, width = q_decayed.shape
    maps = jnp.einsum("hnce,hncd->hned", solved, k_decayed, precision=HIGH)
    identity = jnp.eye(width, dtype=jnp.float32)
    maps = jnp.concatenate(
        [
            identity * jnp.exp(log_last)[..., None, None] - maps[:, :, :width],
            maps[:, :, width:],
        ],
        axis=2,
    )
    joined = inclusive(maps, width)
    start = starts_of(joined[:, -1])
    mixed = jnp.einsum("hncs,hnsd->hncd", scores, solved, precision=HIGH)
    reads = q_decayed - mixed[..., :width]
    later = jnp.einsum("hed,hndf->hnef", start, joined[:, :-1, :width], precision=HIGH)
    states = jnp.concatenate([start[:, None], later + joined[:, :-1, width:]], axis=1)
    result = mixed[..., width:] + jnp.einsum("hncd,hned->hnce", reads, states, precision=HIGH)
    return result.transpose(1, 2, 0, 3).reshape(number * span, heads, width)


def finish(head_mix, output_gate_values, per_head_norm_gain):
    length, heads, width = head_mix.shape
    scaled = head_mix * lax.rsqrt(jnp.mean(head_mix * head_mix, axis=-1, keepdims=True) + EPS)
    gated = (
        scaled
        * per_head_norm_gain
        * jax.nn.silu(output_gate_values.astype(jnp.float32).reshape(length, heads, width))
    )
    return gated.reshape(length, heads * width).astype(jnp.bfloat16)


def normalize(stream, gain):
    wide = stream.astype(jnp.float32)
    return (wide * lax.rsqrt(jnp.mean(wide * wide, axis=-1, keepdims=True) + EPS) * gain).astype(
        jnp.bfloat16
    )


def lookup(table, index):
    found = table[0]
    for place in range(1, len(table)):
        found = jnp.where(index == place, table[place], found)
    return found


def relay_orders(count):
    arrive, leave, when = [], [], []
    for me in range(count):
        others = [s for s in range(count) if s != me]
        middle = (count - 1) / 2
        arrive.append(sorted(others, key=lambda s: (abs(s - me), abs(s - middle))))

        def key(d):
            reach = (count - 1 - d) if me > d else d
            return (reach, reach - abs(me - d))

        order = sorted(others, key=key)
        leave.append(order)
        steps, latest = [], 0
        for d in order:
            latest = max(latest, arrive[me].index(d) + 1)
            steps.append(latest)
        when.append(steps)
    return arrive, leave, when


def experts_kernel(
    count,
    ring,
    room,
    pieces,
    x_ref,
    attended_ref,
    info_ref,
    gate_hbm,
    up_hbm,
    down_hbm,
    common_gate_hbm,
    common_up_hbm,
    common_down_hbm,
    out_ref,
    held,
    tables,
    outbox,
    inbox,
    backbox,
    relay,
    part,
    total,
    hidden,
    picks,
    shares,
    gate,
    up,
    down,
    common_gate,
    common_up,
    common_down,
    weight_sem,
    info_send,
    info_recv,
    hold_send,
    hold_recv,
    go_send,
    go_recv,
    back_send,
    back_recv,
    relay_send,
    relay_recv,
):
    length, width = x_ref.shape
    tp_size = lax.axis_size("tp")
    inner = lax.axis_size("sp") // count
    sp = lax.axis_index("sp")
    outer = sp // inner
    mine = lax.rem(sp, inner) * tp_size + lax.axis_index("tp")
    MESH = pl.DeviceIdType.MESH
    piece = length // pieces
    slots = ring * room
    arrive, leave, when = relay_orders(count)

    def device(o, i):
        return {"sp": o * inner + i // tp_size, "tp": lax.rem(i, tp_size)}

    loads = []
    for n, (src, dst) in enumerate(
        (
            (common_gate_hbm, common_gate),
            (common_up_hbm, common_up),
            (common_down_hbm, common_down),
            (gate_hbm, gate),
            (up_hbm, up),
            (down_hbm, down),
        )
    ):
        load = pltpu.make_async_copy(src, dst, weight_sem.at[n])
        load.start()
        loads.append(load)

    barrier = pltpu.get_barrier_semaphore()
    for step in range(1, count):
        pl.semaphore_signal(
            barrier, inc=1, device_id=device(lax.rem(outer + step, count), mine), device_id_type=MESH
        )
    for step in range(1, ring):
        pl.semaphore_signal(
            barrier, inc=1, device_id=device(outer, lax.rem(mine + step, ring)), device_id_type=MESH
        )
    pl.semaphore_wait(barrier, count + ring - 2)

    def remote(src, dst, send, recv, o, i):
        return pltpu.make_async_remote_copy(
            src_ref=src,
            dst_ref=dst,
            send_sem=send,
            recv_sem=recv,
            device_id=device(o, i),
            device_id_type=MESH,
        )

    info_copies = []
    for step in range(1, count):
        peer = lax.rem(outer + step, count)
        copy = remote(
            info_ref.at[peer], tables.at[outer], info_send.at[step], info_recv.at[step], peer, mine
        )
        copy.start()
        info_copies.append(copy)

    def rows_of(c, size):
        return pl.ds(c * size, size)

    has_right = outer + 1 < count
    has_left = outer > 0

    def own_copy(c, right):
        rows = rows_of(c, piece)
        target = outer + 1 if right else outer - 1
        sem = hold_send.at[count, c] if right else hold_send.at[outer, c]
        return remote(x_ref.at[rows], held.at[outer, rows], sem, hold_recv.at[outer, c], target, mine)

    for c in range(pieces):

        @pl.when(has_right)
        def _():
            own_copy(c, True).start()

        @pl.when(has_left)
        def _():
            own_copy(c, False).start()

    held[outer] = x_ref[...]
    tables[outer] = info_ref[outer]

    def matched(source):
        slot = tables[source, :ring, :]
        place = lax.broadcasted_iota(jnp.int32, (ring, room, length), 1).astype(jnp.float32)
        return slot[:, None, :] == place

    def go_copy(j, source, step):
        peer = lax.rem(mine + step, ring)
        rows = pl.ds(pl.multiple_of(peer * room, room), room)
        mine_rows = pl.ds(pl.multiple_of(mine * room, room), room)
        return remote(
            outbox.at[source, rows],
            inbox.at[source, mine_rows],
            go_send.at[j, step],
            go_recv.at[j, step],
            outer,
            peer,
        )

    def back_copy(j, source, step):
        peer = lax.rem(mine + step, ring)
        rows = pl.ds(pl.multiple_of(peer * room, room), room)
        mine_rows = pl.ds(pl.multiple_of(mine * room, room), room)
        return remote(
            inbox.at[source, rows],
            backbox.at[source, mine_rows],
            back_send.at[j, step],
            back_recv.at[j, step],
            outer,
            peer,
        )

    def spread(j, source):
        picks[...] = (
            jnp.where(matched(source), 1.0, 0.0).reshape(slots, length).astype(jnp.bfloat16)
        )
        tile = min(512, width)

        def body(n, carry):
            cols = pl.ds(pl.multiple_of(n * tile, tile), tile)
            outbox[source, :, cols] = jnp.dot(
                picks[...], held[source, :, cols], preferred_element_type=jnp.float32
            ).astype(jnp.bfloat16)
            return carry

        lax.fori_loop(0, width // tile, body, 0)
        for step in range(1, ring):
            go_copy(j, source, step).start()
        mine_rows = pl.ds(pl.multiple_of(mine * room, room), room)
        inbox[source, mine_rows, :] = outbox[source, mine_rows, :]

    def feed(rows_ref, count_rows, w_gate, w_up, w_down, store):
        inside = w_gate.shape[1]
        tile = min(256, inside)

        def first(n, carry):
            cols = pl.ds(pl.multiple_of(n * tile, tile), tile)
            rows = rows_ref[...]
            gated = jnp.dot(rows, w_gate[:, cols], preferred_element_type=jnp.float32)
            lifted = jnp.dot(rows, w_up[:, cols], preferred_element_type=jnp.float32)
            hidden[pl.ds(0, count_rows), cols] = (gated * jax.nn.sigmoid(gated) * lifted).astype(
                jnp.bfloat16
            )
            return carry

        lax.fori_loop(0, inside // tile, first, 0)
        wide = min(512, width)

        def second(n, carry):
            cols = pl.ds(pl.multiple_of(n * wide, wide), wide)
            store(
                cols,
                jnp.dot(
                    hidden[pl.ds(0, count_rows), :],
                    w_down[:, cols],
                    preferred_element_type=jnp.float32,
                ),
            )
            return carry

        lax.fori_loop(0, width // wide, second, 0)

    def serve(j, source):
        for step in range(1, ring):
            go_copy(j, source, step).wait_recv()

        def store(cols, value):
            inbox[source, :, cols] = value.astype(jnp.bfloat16)

        feed(inbox.at[source], slots, gate, up, down, store)

    def send_back(j, source):
        for step in range(1, ring):
            back_copy(j, source, step).start()
        mine_rows = pl.ds(pl.multiple_of(mine * room, room), room)
        backbox[source, mine_rows, :] = inbox[source, mine_rows, :]

    def combine(j, source, store):
        weight = tables[source, ring:, :]
        spread_weight = jnp.where(matched(source), weight[:, None, :], 0.0).reshape(slots, length)
        turned = spread_weight.T
        high = turned.astype(jnp.bfloat16)
        shares[0] = high
        shares[1] = (turned - high.astype(jnp.float32)).astype(jnp.bfloat16)
        for step in range(1, ring):
            back_copy(j, source, step).wait_recv()
        tile = min(512, width)

        def body(n, carry):
            cols = pl.ds(pl.multiple_of(n * tile, tile), tile)
            rows = backbox[source, :, cols]
            store(
                cols,
                jnp.dot(shares[0], rows, preferred_element_type=jnp.float32)
                + jnp.dot(shares[1], rows, preferred_element_type=jnp.float32),
            )
            return carry

        lax.fori_loop(0, width // tile, body, 0)

    def forward_copy(source, c):
        rows = rows_of(c, piece)
        target = jnp.where(source < outer, outer + 1, outer - 1)
        return remote(
            held.at[source, rows],
            held.at[source, rows],
            hold_send.at[jnp.where(source < outer, source, source), c],
            hold_recv.at[source, c],
            target,
            mine,
        )

    def goes_on(source):
        return ((source < outer) & has_right) | ((source > outer) & has_left)

    def receive(source):
        for c in range(pieces):
            forward_copy(source, c).wait_recv()

            @pl.when(goes_on(source))
            def _():
                forward_copy(source, c).start()

    def relay_copy(dest, c):
        rows = rows_of(c, piece)
        leftward = dest < outer
        target = jnp.where(leftward, outer - 1, outer + 1)
        landing = jnp.where(leftward & (target == dest), count, dest)
        return remote(
            relay.at[dest, rows],
            relay.at[landing, rows],
            relay_send.at[dest, c],
            relay_recv.at[landing, c],
            target,
            mine,
        )

    def landed(place, c):
        rows = rows_of(c, piece)
        return remote(
            relay.at[place, rows],
            relay.at[place, rows],
            relay_send.at[0, c],
            relay_recv.at[place, c],
            lax.rem(outer + 1, count),
            mine,
        )

    def pass_on(dest):
        upstream = ((dest < outer) & has_right) | ((dest > outer) & has_left)
        for c in range(pieces):
            rows = rows_of(c, piece)

            @pl.when(upstream)
            def _():
                landed(dest, c).wait_recv()
                relay[dest, rows, :] = (
                    relay[dest, rows, :].astype(jnp.float32) + part[dest, rows, :]
                ).astype(jnp.bfloat16)

            @pl.when(jnp.logical_not(upstream))
            def _():
                relay[dest, rows, :] = part[dest, rows, :].astype(jnp.bfloat16)

            relay_copy(dest, c).start()

    order = [outer] + [lookup([arrive[m][j] for m in range(count)], outer) for j in range(count - 1)]
    drain = [lookup([leave[m][j] for m in range(count)], outer) for j in range(count - 1)]

    spread(0, outer)
    for load in loads[:3]:
        load.wait()

    def keep(cols, value):
        total[:, cols] = attended_ref[:, cols].astype(jnp.float32) + value

    feed(x_ref, length, common_gate, common_up, common_down, keep)
    for copy in info_copies:
        copy.wait_recv()

    def store_part(source):
        def store(cols, value):
            part[source, :, cols] = value

        return store

    def collect(j):
        combine(j, order[j], store_part(order[j]))
        for k in range(count - 1):
            places = [when[m][k] for m in range(count)]
            if j in places:
                if all(p == j for p in places):
                    pass_on(drain[k])
                else:

                    @pl.when(lookup([int(p == j) for p in places], outer) == 1)
                    def _():
                        pass_on(drain[k])

    for j in range(1, count):
        if j == 2:
            serve(1, order[1])
            send_back(1, order[1])
        receive(order[j])
        spread(j, order[j])
        if j == 1:
            for load in loads[3:]:
                load.wait()
            serve(0, order[0])
        if j > 2:
            serve(j - 1, order[j - 1])
            send_back(j - 1, order[j - 1])
            collect(j - 2)
    last = count - 1
    if last == 1 or last > 1:
        serve(last, order[last])
        send_back(last, order[last])
    send_back(0, order[0])
    if last > 1:
        collect(last - 1)
    collect(last)

    def add(cols, value):
        total[:, cols] += value

    combine(0, order[0], add)
    for side, place in ((has_left, outer), (has_right, count)):
        for c in range(pieces):
            rows = rows_of(c, piece)

            @pl.when(side)
            def _():
                landed(place, c).wait_recv()
                total[rows, :] += relay[place, rows, :].astype(jnp.float32)

    out_ref[...] = total[...].astype(jnp.bfloat16)

    for copy in info_copies:
        copy.wait_send()
    for c in range(pieces):

        @pl.when(has_right)
        def _():
            own_copy(c, True).wait_send()

        @pl.when(has_left)
        def _():
            own_copy(c, False).wait_send()

    for j in range(count):
        if j > 0:
            for c in range(pieces):

                @pl.when(goes_on(order[j]))
                def _():
                    forward_copy(order[j], c).wait_send()

                relay_copy(order[j], c).wait_send()
        for step in range(1, ring):
            go_copy(j, order[j], step).wait_send()
            back_copy(j, order[j], step).wait_send()


def outer_size(size):
    bits = size.bit_length() - 1
    return 1 << -(-bits // 3)


def experts_part(
    normed,
    attended,
    info,
    count,
    ring,
    room,
    weights,
    identity,
):
    length, width = normed.shape
    inside = weights[0].shape[1]
    shared = weights[3].shape[1]
    pieces = 4
    slots = ring * room
    bf16 = jnp.bfloat16
    vmem = pl.BlockSpec(memory_space=pltpu.VMEM)
    anywhere = pl.BlockSpec(memory_space=pl.ANY)
    dma = pltpu.SemaphoreType.DMA
    return pl.pallas_call(
        functools.partial(experts_kernel, count, ring, room, pieces),
        name="experts",
        out_shape=jax.ShapeDtypeStruct((length, width), bf16),
        in_specs=[vmem] * 3 + [anywhere] * 6,
        out_specs=vmem,
        scratch_shapes=[
            pltpu.VMEM((count, length, width), bf16),
            pltpu.VMEM((count,) + info.shape[1:], jnp.float32),
            pltpu.VMEM((count, slots, width), bf16),
            pltpu.VMEM((count, slots, width), bf16),
            pltpu.VMEM((count, slots, width), bf16),
            pltpu.VMEM((count + 1, length, width), bf16),
            pltpu.VMEM((count, length, width), jnp.float32),
            pltpu.VMEM((length, width), jnp.float32),
            pltpu.VMEM((max(slots, length), max(inside, shared)), bf16),
            pltpu.VMEM((slots, length), bf16),
            pltpu.VMEM((2, length, slots), bf16),
        ]
        + [pltpu.VMEM(w.shape, w.dtype) for w in weights]
        + [
            dma((6,)),
            dma((count,)),
            dma((count,)),
            dma((count + 1, pieces)),
            dma((count, pieces)),
            dma((count, ring)),
            dma((count, ring)),
            dma((count, ring)),
            dma((count, ring)),
            dma((count, pieces)),
            dma((count + 1, pieces)),
        ],
        compiler_params=pltpu.CompilerParams(
            collective_id=identity, has_side_effects=True, vmem_limit_bytes=67043328
        ),
    )(normed, attended, info, *weights)


def shards(
    projected_queries,
    projected_keys,
    projected_values,
    output_gate_values,
    write_strength_logits,
    decay_input_logits,
    head_rate_logarithm,
    extra_log_decay,
    per_head_norm_gain,
    output_matrix,
    residual,
    mixture_norm_gain,
    selected_expert_index,
    routing_weight,
    routed_gate_weight,
    routed_up_weight,
    routed_down_weight,
    common_gate_weight,
    common_up_weight,
    common_down_weight,
):
    prepared_inputs = prepare_inputs(
        projected_queries,
        projected_keys,
        projected_values,
        write_strength_logits,
        decay_input_logits,
        head_rate_logarithm,
        extra_log_decay,
    )
    terms = block_terms(*prepared_inputs)
    heads_out = finish(mix_heads(terms), output_gate_values, per_head_norm_gain)
    token_heads = lax.all_to_all(heads_out, "tp", split_axis=0, concat_axis=1, tiled=True)
    projected = jnp.dot(token_heads, output_matrix, preferred_element_type=jnp.float32)
    attended = (residual.astype(jnp.float32) + projected).astype(jnp.bfloat16)
    normed = normalize(attended, mixture_norm_gain)
    length = normed.shape[0]
    tp_size = lax.axis_size("tp")
    sp_size = lax.axis_size("sp")
    experts = sp_size * tp_size
    count = outer_size(sp_size)
    ring = experts // count
    room = max(2, length * TOP_K * 3 // (2 * experts))
    room = -(-room // 16) * 16
    chosen = selected_expert_index[:, :, None] == jnp.arange(experts, dtype=jnp.int32)
    named = jnp.any(chosen, axis=1)
    weight = jnp.sum(jnp.where(chosen, routing_weight[:, :, None], 0.0), axis=1)
    place = jnp.arange(length, dtype=jnp.int32)
    earlier = (place[:, None] > place[None, :]).astype(jnp.bfloat16)
    slot = jnp.dot(earlier, named.astype(jnp.bfloat16), preferred_element_type=jnp.float32)
    slot = jnp.where(named, slot, float(room))
    info = jnp.concatenate(
        [slot.T.reshape(count, ring, length), weight.T.reshape(count, ring, length)], axis=1
    )
    weights = (
        routed_gate_weight[0],
        routed_up_weight[0],
        routed_down_weight[0],
        common_gate_weight,
        common_up_weight,
        common_down_weight,
    )
    return experts_part(normed, attended, info, count, ring, room, weights, 2)


def solution(mesh):
    return jax.shard_map(
        shards,
        mesh=mesh,
        in_specs=(
            P("sp", "tp"),
            P("sp", "tp"),
            P("sp", "tp"),
            P("sp", "tp"),
            P("sp", "tp"),
            P("sp", "tp"),
            P("tp"),
            P("sp", "tp"),
            P(),
            P(),
            P(("sp", "tp"), None),
            P(),
            P(("sp", "tp"), None),
            P(("sp", "tp"), None),
            P(("sp", "tp"), None, None),
            P(("sp", "tp"), None, None),
            P(("sp", "tp"), None, None),
            P(),
            P(),
            P(),
        ),
        out_specs=P(("sp", "tp"), None),
        check_vma=False,
    )
```

```python
import functools

import jax
import jax.numpy as jnp
from jax import lax
from jax.experimental import pallas as pl
from jax.experimental.pallas import tpu as pltpu
from jax.sharding import PartitionSpec as P

TOP_K = 4
SPAN = 64


EPS = 1e-06
HIGH = lax.Precision.HIGHEST


def halves(x):
    high = x.astype(jnp.bfloat16)
    return high, (x - high.astype(jnp.float32)).astype(jnp.bfloat16)


NN = (((1,), (0,)), ((), ()))
NT = (((1,), (1,)), ((), ()))


def once(a, b, dims=NN):
    return lax.dot_general(
        a.astype(jnp.bfloat16), b.astype(jnp.bfloat16), dims, preferred_element_type=jnp.float32
    )


def thrice(a, b, dims=NN):
    a_high, a_low = halves(a)
    b_high, b_low = halves(b)

    def dot(x, y):
        return lax.dot_general(x, y, dims, preferred_element_type=jnp.float32)

    return dot(a_high, b_high) + (dot(a_high, b_low) + dot(a_low, b_high))


def silu(x):
    return x * jax.nn.sigmoid(x)


def heads_kernel(
    count,
    span,
    q_ref,
    k_ref,
    v_ref,
    gate_ref,
    small_ref,
    gain_ref,
    residual_ref,
    mixture_gain_ref,
    matrix_hbm,
    normed_ref,
    attended_ref,
    erase,
    fresh,
    score,
    reads,
    late,
    maps,
    fade,
    gathered,
    prefix,
    carried,
    starting,
    start,
    mixed,
    finished,
    token_heads,
    matrix,
    matrix_sem,
    ring_send,
    ring_recv,
    line_send,
    line_recv,
    home_send,
    home_recv,
    pair_send,
    pair_recv,
):
    f32 = jnp.float32
    length, columns = q_ref.shape
    heads, number = erase.shape[:2]
    width = columns // heads
    tp_size = lax.axis_size("tp")
    members = lax.axis_size("sp") // count
    parts = members // heads
    slab = width // parts
    sp = lax.axis_index("sp")
    tp = lax.axis_index("tp")
    outer = sp // members
    member = lax.rem(sp, members)
    MESH = pl.DeviceIdType.MESH
    own = length // tp_size

    load = pltpu.make_async_copy(matrix_hbm, matrix, matrix_sem)
    load.start()

    def device(o, m, t):
        return {"sp": o * members + m, "tp": t}

    barrier = pltpu.get_barrier_semaphore()

    def greet(where):
        pl.semaphore_signal(barrier, inc=1, device_id=where, device_id_type=MESH)

    for step in range(1, count):
        greet(device(lax.rem(outer + step, count), member, tp))
    for step in range(1, members):
        greet(device(outer, lax.rem(member + step, members), tp))
    for step in range(1, tp_size):
        greet(device(outer, member, lax.rem(tp + step, tp_size)))

    row = lax.broadcasted_iota(jnp.int32, (span, span), 0)
    column = lax.broadcasted_iota(jnp.int32, (span, span), 1)
    causal = row >= column
    strict = row > column
    one = (row == column).astype(f32)
    lower = causal.astype(f32)
    group = 2 if number % 2 == 0 else 1

    def prepare(it, carry):
        jobs = []
        for part in range(group):
            c = it * group + part
            rows = pl.ds(pl.multiple_of(c * span, span), span)
            small = small_ref[rows, :]
            summed = jnp.dot(
                lower, small, precision=HIGH, preferred_element_type=f32
            )
            turned = summed.T
            for h in range(heads):
                cols = slice(h * width, (h + 1) * width)
                q = silu(q_ref[rows, cols].astype(f32))
                q = q * lax.rsqrt(jnp.sum(q * q, axis=-1, keepdims=True) + EPS)
                k = silu(k_ref[rows, cols].astype(f32))
                k = k * lax.rsqrt(jnp.sum(k * k, axis=-1, keepdims=True) + EPS)
                beta = small[:, h : h + 1]
                g_column = summed[:, heads + h : heads + h + 1]
                g_row = turned[heads + h : heads + h + 1, :]
                decay = jnp.where(
                    causal, jnp.exp(jnp.where(causal, g_column - g_row, 0.0)), 0.0
                )
                kb = k * beta
                both = thrice(jnp.concatenate([kb, q], axis=0), k, NT)
                below = jnp.where(strict, both[:span] * decay, 0.0)
                score[h, c] = both[span:] * decay
                grown = jnp.exp(g_column)
                reads[h, c] = q * grown
                last = g_column[span - 1 :, :]
                late[h, c] = k * jnp.exp(last - g_column)
                fade[h, c] = jnp.broadcast_to(jnp.exp(last), fade.shape[2:])
                v = silu(v_ref[rows, cols].astype(f32)) * beta
                jobs.append((h, c, below, jnp.concatenate([kb * grown, v], axis=1)))
        found = None
        size = 1
        while size < span:
            pair = (row // size) - (column // size)
            mask = ((row // size) % 2 == 1) & (pair == 1)
            pieces = [jnp.where(mask, job[2], 0.0) for job in jobs]
            if found is None:
                found = [one - piece for piece in pieces]
            else:
                inner = [once(x, piece) for x, piece in zip(found, pieces)]
                found = [x - once(y, x) for x, y in zip(found, inner)]
            size *= 2
        wrong = [one - x - thrice(job[2], x) for x, job in zip(found, jobs)]
        found = [x + once(x, e) for x, e in zip(found, wrong)]
        for x, (h, c, _, right) in zip(found, jobs):
            solved = thrice(x, right)
            erase[h, c] = solved[:, :width]
            fresh[h, c] = solved[:, width:].T
        return carry

    lax.fori_loop(0, number // group, prepare, 0)

    square = (
        lax.broadcasted_iota(jnp.int32, (width, width), 0)
        == lax.broadcasted_iota(jnp.int32, (width, width), 1)
    ).astype(f32)
    for h in range(heads):
        maps[h, pl.ds(0, width), :] = square
        maps[h, pl.ds(width, width), :] = jnp.zeros((width, width), f32)

    def advance(c, carry):
        rows = pl.ds(pl.multiple_of(c * span, span), span)
        for h in range(heads):
            state = maps[h]
            gone = thrice(state, erase[h, c], NT)
            news = jnp.concatenate([-gone[:width], fresh[h, c] - gone[width:]], axis=0)
            mixed[h, rows, :] = thrice(reads[h, c], state, NT) + thrice(score[h, c], news, NT)
            maps[h] = state * fade[h, c, 0:1, :] + thrice(news, late[h, c])
        return carry

    lax.fori_loop(0, number, advance, 0)

    pl.semaphore_wait(barrier, count + members + tp_size - 3)

    def remote(src, dst, send, recv, where):
        return pltpu.make_async_remote_copy(
            src_ref=src,
            dst_ref=dst,
            send_sem=send,
            recv_sem=recv,
            device_id=where,
            device_id_type=MESH,
        )

    def ring_copies(step):
        peer = lax.rem(member + step, members)
        head = peer // parts
        which = lax.rem(peer, parts)
        where = device(outer, peer, tp)
        return (
            remote(
                maps.at[head, pl.ds(0, width)],
                gathered.at[member, pl.ds(0, width)],
                ring_send.at[step, 0],
                ring_recv.at[step, 0],
                where,
            ),
            remote(
                maps.at[head, pl.ds(pl.multiple_of(width + which * slab, slab), slab)],
                gathered.at[member, pl.ds(width, slab)],
                ring_send.at[step, 1],
                ring_recv.at[step, 1],
                where,
            ),
        )

    for step in range(1, members):
        for copy in ring_copies(step):
            copy.start()
    my_head = member // parts
    my_part = lax.rem(member, parts)
    gathered[member, pl.ds(0, width), :] = maps[my_head, pl.ds(0, width), :]
    gathered[member, pl.ds(width, slab), :] = maps[
        my_head, pl.ds(pl.multiple_of(width + my_part * slab, slab), slab), :
    ]
    for step in range(1, members):
        for copy in ring_copies(step):
            copy.wait_recv()

    prefix[0, pl.ds(0, width), :] = square
    prefix[0, pl.ds(width, slab), :] = jnp.zeros((slab, width), f32)
    for r in range(members):
        joined = thrice(prefix[r], gathered[r, pl.ds(0, width), :])
        prefix[r + 1, pl.ds(0, width), :] = joined[:width]
        prefix[r + 1, pl.ds(width, slab), :] = joined[width:] + gathered[r, pl.ds(width, slab), :]

    def line_copy():
        return remote(
            carried.at[1],
            carried.at[0],
            line_send,
            line_recv,
            device(lax.rem(outer + 1, count), member, tp),
        )

    @pl.when(outer == 0)
    def _():
        carried[0] = jnp.zeros((slab, width), f32)

    @pl.when(outer > 0)
    def _():
        line_copy().wait_recv()

    arrived = carried[0]
    carried[1] = (
        thrice(arrived, prefix[members, pl.ds(0, width), :])
        + prefix[members, pl.ds(width, slab), :]
    )

    @pl.when(outer + 1 < count)
    def _():
        line_copy().start()

    for r in range(members):
        starting[r] = (
            thrice(arrived, prefix[r, pl.ds(0, width), :]) + prefix[r, pl.ds(width, slab), :]
        )

    def home_copy(step):
        peer = lax.rem(member + step, members)
        return remote(
            starting.at[peer],
            start.at[my_head, pl.ds(pl.multiple_of(my_part * slab, slab), slab)],
            home_send.at[step],
            home_recv.at[step],
            device(outer, peer, tp),
        )

    def home_landed(step):
        peer = lax.rem(member + members - step, members)
        return remote(
            starting.at[0],
            start.at[peer // parts, pl.ds(pl.multiple_of(lax.rem(peer, parts) * slab, slab), slab)],
            home_send.at[step],
            home_recv.at[step],
            device(outer, lax.rem(member + step, members), tp),
        )

    for step in range(1, members):
        home_copy(step).start()
    start[my_head, pl.ds(pl.multiple_of(my_part * slab, slab), slab), :] = starting[member]
    for step in range(1, members):
        home_landed(step).wait_recv()

    def close(c, carry):
        rows = pl.ds(pl.multiple_of(c * span, span), span)
        for h in range(heads):
            cols = slice(h * width, (h + 1) * width)
            both = mixed[h, rows, :]
            value = both[:, width:] + thrice(both[:, :width], start[h], NT)
            scaled = value * lax.rsqrt(jnp.mean(value * value, axis=-1, keepdims=True) + EPS)
            finished[rows, cols] = (
                scaled * gain_ref[...] * silu(gate_ref[rows, cols].astype(f32))
            ).astype(jnp.bfloat16)
        return carry

    lax.fori_loop(0, number, close, 0)

    def pair_copy(step):
        peer = lax.rem(tp + step, tp_size)
        return remote(
            finished.at[pl.ds(pl.multiple_of(peer * own, own), own)],
            token_heads.at[tp],
            pair_send.at[step],
            pair_recv.at[step],
            device(outer, member, peer),
        )

    for step in range(1, tp_size):
        pair_copy(step).start()
    token_heads[tp] = finished[pl.ds(pl.multiple_of(tp * own, own), own), :]
    load.wait()
    for step in range(1, tp_size):
        pair_copy(step).wait_recv()

    wide = residual_ref.shape[1]
    tile = min(512, wide)
    squares = jnp.zeros((own, 1), f32)
    for n in range(wide // tile):
        cols = slice(n * tile, (n + 1) * tile)
        value = residual_ref[:, cols].astype(f32)
        for t in range(tp_size):
            value += jnp.dot(
                token_heads[t],
                matrix[pl.ds(t * columns, columns), cols],
                preferred_element_type=f32,
            )
        rounded = value.astype(jnp.bfloat16)
        attended_ref[:, cols] = rounded
        again = rounded.astype(f32)
        squares += jnp.sum(again * again, axis=-1, keepdims=True)
    factor = lax.rsqrt(squares / wide + EPS)
    for n in range(wide // tile):
        cols = slice(n * tile, (n + 1) * tile)
        normed_ref[:, cols] = (
            attended_ref[:, cols].astype(f32) * factor * mixture_gain_ref[:, cols]
        ).astype(jnp.bfloat16)

    for step in range(1, members):
        for copy in ring_copies(step):
            copy.wait_send()
        home_copy(step).wait_send()
    for step in range(1, tp_size):
        pair_copy(step).wait_send()

    @pl.when(outer + 1 < count)
    def _():
        line_copy().wait_send()


def heads_part(
    queries, keys, values, gates, small, gain, residual, mixture_gain, matrix, heads, count, identity
):
    length, columns = queries.shape
    width = columns // heads
    own, wide = residual.shape
    tp_size = lax.axis_size("tp")
    members = lax.axis_size("sp") // count
    parts = members // heads
    slab = width // parts
    span = min(2 * SPAN, length)
    number = length // span
    bf16, f32 = jnp.bfloat16, jnp.float32
    vmem = pl.BlockSpec(memory_space=pltpu.VMEM)
    dma = pltpu.SemaphoreType.DMA
    return pl.pallas_call(
        functools.partial(heads_kernel, count, span),
        name="heads",
        out_shape=[jax.ShapeDtypeStruct((own, wide), bf16)] * 2,
        in_specs=[vmem] * 8 + [pl.BlockSpec(memory_space=pl.ANY)],
        out_specs=[vmem] * 2,
        scratch_shapes=[
            pltpu.VMEM((heads, number, span, width), f32),
            pltpu.VMEM((heads, number, width, span), f32),
            pltpu.VMEM((heads, number, span, span), f32),
            pltpu.VMEM((heads, number, span, width), f32),
            pltpu.VMEM((heads, number, span, width), f32),
            pltpu.VMEM((heads, 2 * width, width), f32),
            pltpu.VMEM((heads, number, 8, width), f32),
            pltpu.VMEM((members, width + slab, width), f32),
            pltpu.VMEM((members + 1, width + slab, width), f32),
            pltpu.VMEM((2, slab, width), f32),
            pltpu.VMEM((members, slab, width), f32),
            pltpu.VMEM((heads, width, width), f32),
            pltpu.VMEM((heads, length, 2 * width), f32),
            pltpu.VMEM((length, columns), bf16),
            pltpu.VMEM((tp_size, own, columns), bf16),
            pltpu.VMEM(matrix.shape, matrix.dtype),
            dma,
            dma((members, 2)),
            dma((members, 2)),
            dma,
            dma,
            dma((members,)),
            dma((members,)),
            dma((tp_size,)),
            dma((tp_size,)),
        ],
        compiler_params=pltpu.CompilerParams(
            collective_id=identity, has_side_effects=True, vmem_limit_bytes=60000000
        ),
    )(queries, keys, values, gates, small, gain, residual, mixture_gain, matrix)


def lookup(table, index):
    found = table[0]
    for place in range(1, len(table)):
        found = jnp.where(index == place, table[place], found)
    return found


def relay_orders(count):
    arrive, leave, when = [], [], []
    for me in range(count):
        others = [s for s in range(count) if s != me]
        middle = (count - 1) / 2
        arrive.append(sorted(others, key=lambda s: (abs(s - me), abs(s - middle))))

        def key(d):
            reach = (count - 1 - d) if me > d else d
            return (reach, reach - abs(me - d))

        order = sorted(others, key=key)
        leave.append(order)
        steps, latest = [], 0
        for d in order:
            latest = max(latest, arrive[me].index(d) + 1)
            steps.append(latest)
        when.append(steps)
    return arrive, leave, when


def experts_kernel(
    count,
    ring,
    room,
    pieces,
    x_ref,
    attended_ref,
    info_ref,
    gate_hbm,
    up_hbm,
    down_hbm,
    common_gate_hbm,
    common_up_hbm,
    common_down_hbm,
    out_ref,
    held,
    tables,
    outbox,
    inbox,
    backbox,
    relay,
    part,
    total,
    hidden,
    picks,
    shares,
    gate,
    up,
    down,
    common_gate,
    common_up,
    common_down,
    weight_sem,
    info_send,
    info_recv,
    hold_send,
    hold_recv,
    go_send,
    go_recv,
    back_send,
    back_recv,
    relay_send,
    relay_recv,
):
    length, width = x_ref.shape
    tp_size = lax.axis_size("tp")
    inner = lax.axis_size("sp") // count
    sp = lax.axis_index("sp")
    outer = sp // inner
    mine = lax.rem(sp, inner) * tp_size + lax.axis_index("tp")
    MESH = pl.DeviceIdType.MESH
    piece = length // pieces
    slots = ring * room
    arrive, leave, when = relay_orders(count)

    def device(o, i):
        return {"sp": o * inner + i // tp_size, "tp": lax.rem(i, tp_size)}

    loads = []
    for n, (src, dst) in enumerate(
        (
            (common_gate_hbm, common_gate),
            (common_up_hbm, common_up),
            (common_down_hbm, common_down),
            (gate_hbm, gate),
            (up_hbm, up),
            (down_hbm, down),
        )
    ):
        load = pltpu.make_async_copy(src, dst, weight_sem.at[n])
        load.start()
        loads.append(load)

    barrier = pltpu.get_barrier_semaphore()
    for step in range(1, count):
        pl.semaphore_signal(
            barrier, inc=1, device_id=device(lax.rem(outer + step, count), mine), device_id_type=MESH
        )
    for step in range(1, ring):
        pl.semaphore_signal(
            barrier, inc=1, device_id=device(outer, lax.rem(mine + step, ring)), device_id_type=MESH
        )
    pl.semaphore_wait(barrier, count + ring - 2)

    def remote(src, dst, send, recv, o, i):
        return pltpu.make_async_remote_copy(
            src_ref=src,
            dst_ref=dst,
            send_sem=send,
            recv_sem=recv,
            device_id=device(o, i),
            device_id_type=MESH,
        )

    info_copies = []
    for step in range(1, count):
        peer = lax.rem(outer + step, count)
        copy = remote(
            info_ref.at[peer], tables.at[outer], info_send.at[step], info_recv.at[step], peer, mine
        )
        copy.start()
        info_copies.append(copy)

    def rows_of(c, size):
        return pl.ds(c * size, size)

    has_right = outer + 1 < count
    has_left = outer > 0

    def own_copy(c, right):
        rows = rows_of(c, piece)
        target = outer + 1 if right else outer - 1
        sem = hold_send.at[count, c] if right else hold_send.at[outer, c]
        return remote(x_ref.at[rows], held.at[outer, rows], sem, hold_recv.at[outer, c], target, mine)

    for c in range(pieces):

        @pl.when(has_right)
        def _():
            own_copy(c, True).start()

        @pl.when(has_left)
        def _():
            own_copy(c, False).start()

    held[outer] = x_ref[...]
    tables[outer] = info_ref[outer]

    def matched(source):
        slot = tables[source, :ring, :]
        place = lax.broadcasted_iota(jnp.int32, (ring, room, length), 1).astype(jnp.float32)
        return slot[:, None, :] == place

    def go_copy(j, source, step):
        peer = lax.rem(mine + step, ring)
        rows = pl.ds(pl.multiple_of(peer * room, room), room)
        mine_rows = pl.ds(pl.multiple_of(mine * room, room), room)
        return remote(
            outbox.at[source, rows],
            inbox.at[source, mine_rows],
            go_send.at[j, step],
            go_recv.at[j, step],
            outer,
            peer,
        )

    def back_copy(j, source, step):
        peer = lax.rem(mine + step, ring)
        rows = pl.ds(pl.multiple_of(peer * room, room), room)
        mine_rows = pl.ds(pl.multiple_of(mine * room, room), room)
        return remote(
            inbox.at[source, rows],
            backbox.at[source, mine_rows],
            back_send.at[j, step],
            back_recv.at[j, step],
            outer,
            peer,
        )

    def spread(j, source):
        picks[...] = (
            jnp.where(matched(source), 1.0, 0.0).reshape(slots, length).astype(jnp.bfloat16)
        )
        tile = min(512, width)

        def body(n, carry):
            cols = pl.ds(pl.multiple_of(n * tile, tile), tile)
            outbox[source, :, cols] = jnp.dot(
                picks[...], held[source, :, cols], preferred_element_type=jnp.float32
            ).astype(jnp.bfloat16)
            return carry

        lax.fori_loop(0, width // tile, body, 0)
        for step in range(1, ring):
            go_copy(j, source, step).start()
        mine_rows = pl.ds(pl.multiple_of(mine * room, room), room)
        inbox[source, mine_rows, :] = outbox[source, mine_rows, :]

    def feed(rows_ref, count_rows, w_gate, w_up, w_down, store):
        inside = w_gate.shape[1]
        tile = min(256, inside)

        def first(n, carry):
            cols = pl.ds(pl.multiple_of(n * tile, tile), tile)
            rows = rows_ref[...]
            gated = jnp.dot(rows, w_gate[:, cols], preferred_element_type=jnp.float32)
            lifted = jnp.dot(rows, w_up[:, cols], preferred_element_type=jnp.float32)
            hidden[pl.ds(0, count_rows), cols] = (gated * jax.nn.sigmoid(gated) * lifted).astype(
                jnp.bfloat16
            )
            return carry

        lax.fori_loop(0, inside // tile, first, 0)
        wide = min(512, width)

        def second(n, carry):
            cols = pl.ds(pl.multiple_of(n * wide, wide), wide)
            store(
                cols,
                jnp.dot(
                    hidden[pl.ds(0, count_rows), :],
                    w_down[:, cols],
                    preferred_element_type=jnp.float32,
                ),
            )
            return carry

        lax.fori_loop(0, width // wide, second, 0)

    def serve(j, source):
        for step in range(1, ring):
            go_copy(j, source, step).wait_recv()

        def store(cols, value):
            inbox[source, :, cols] = value.astype(jnp.bfloat16)

        feed(inbox.at[source], slots, gate, up, down, store)

    def send_back(j, source):
        for step in range(1, ring):
            back_copy(j, source, step).start()
        mine_rows = pl.ds(pl.multiple_of(mine * room, room), room)
        backbox[source, mine_rows, :] = inbox[source, mine_rows, :]

    def combine(j, source, store):
        weight = tables[source, ring:, :]
        spread_weight = jnp.where(matched(source), weight[:, None, :], 0.0).reshape(slots, length)
        turned = spread_weight.T
        high = turned.astype(jnp.bfloat16)
        shares[0] = high
        shares[1] = (turned - high.astype(jnp.float32)).astype(jnp.bfloat16)
        for step in range(1, ring):
            back_copy(j, source, step).wait_recv()
        tile = min(512, width)

        def body(n, carry):
            cols = pl.ds(pl.multiple_of(n * tile, tile), tile)
            rows = backbox[source, :, cols]
            store(
                cols,
                jnp.dot(shares[0], rows, preferred_element_type=jnp.float32)
                + jnp.dot(shares[1], rows, preferred_element_type=jnp.float32),
            )
            return carry

        lax.fori_loop(0, width // tile, body, 0)

    def forward_copy(source, c):
        rows = rows_of(c, piece)
        target = jnp.where(source < outer, outer + 1, outer - 1)
        return remote(
            held.at[source, rows],
            held.at[source, rows],
            hold_send.at[jnp.where(source < outer, source, source), c],
            hold_recv.at[source, c],
            target,
            mine,
        )

    def goes_on(source):
        return ((source < outer) & has_right) | ((source > outer) & has_left)

    def receive(source):
        for c in range(pieces):
            forward_copy(source, c).wait_recv()

            @pl.when(goes_on(source))
            def _():
                forward_copy(source, c).start()

    def relay_copy(dest, c):
        rows = rows_of(c, piece)
        leftward = dest < outer
        target = jnp.where(leftward, outer - 1, outer + 1)
        landing = jnp.where(leftward & (target == dest), count, dest)
        return remote(
            relay.at[dest, rows],
            relay.at[landing, rows],
            relay_send.at[dest, c],
            relay_recv.at[landing, c],
            target,
            mine,
        )

    def landed(place, c):
        rows = rows_of(c, piece)
        return remote(
            relay.at[place, rows],
            relay.at[place, rows],
            relay_send.at[0, c],
            relay_recv.at[place, c],
            lax.rem(outer + 1, count),
            mine,
        )

    def pass_on(dest):
        upstream = ((dest < outer) & has_right) | ((dest > outer) & has_left)
        for c in range(pieces):
            rows = rows_of(c, piece)

            @pl.when(upstream)
            def _():
                landed(dest, c).wait_recv()
                relay[dest, rows, :] = (
                    relay[dest, rows, :].astype(jnp.float32) + part[dest, rows, :]
                ).astype(jnp.bfloat16)

            @pl.when(jnp.logical_not(upstream))
            def _():
                relay[dest, rows, :] = part[dest, rows, :].astype(jnp.bfloat16)

            relay_copy(dest, c).start()

    order = [outer] + [lookup([arrive[m][j] for m in range(count)], outer) for j in range(count - 1)]
    drain = [lookup([leave[m][j] for m in range(count)], outer) for j in range(count - 1)]

    spread(0, outer)
    for load in loads[:3]:
        load.wait()

    def keep(cols, value):
        total[:, cols] = attended_ref[:, cols].astype(jnp.float32) + value

    feed(x_ref, length, common_gate, common_up, common_down, keep)
    for copy in info_copies:
        copy.wait_recv()

    def store_part(source):
        def store(cols, value):
            part[source, :, cols] = value

        return store

    def collect(j):
        combine(j, order[j], store_part(order[j]))
        for k in range(count - 1):
            places = [when[m][k] for m in range(count)]
            if j in places:
                if all(p == j for p in places):
                    pass_on(drain[k])
                else:

                    @pl.when(lookup([int(p == j) for p in places], outer) == 1)
                    def _():
                        pass_on(drain[k])

    for j in range(1, count):
        if j == 2:
            serve(1, order[1])
            send_back(1, order[1])
        receive(order[j])
        spread(j, order[j])
        if j == 1:
            for load in loads[3:]:
                load.wait()
            serve(0, order[0])
        if j > 2:
            serve(j - 1, order[j - 1])
            send_back(j - 1, order[j - 1])
            collect(j - 2)
    last = count - 1
    if last == 1 or last > 1:
        serve(last, order[last])
        send_back(last, order[last])
    send_back(0, order[0])
    if last > 1:
        collect(last - 1)
    collect(last)

    def add(cols, value):
        total[:, cols] += value

    combine(0, order[0], add)
    for side, place in ((has_left, outer), (has_right, count)):
        for c in range(pieces):
            rows = rows_of(c, piece)

            @pl.when(side)
            def _():
                landed(place, c).wait_recv()
                total[rows, :] += relay[place, rows, :].astype(jnp.float32)

    out_ref[...] = total[...].astype(jnp.bfloat16)

    for copy in info_copies:
        copy.wait_send()
    for c in range(pieces):

        @pl.when(has_right)
        def _():
            own_copy(c, True).wait_send()

        @pl.when(has_left)
        def _():
            own_copy(c, False).wait_send()

    for j in range(count):
        if j > 0:
            for c in range(pieces):

                @pl.when(goes_on(order[j]))
                def _():
                    forward_copy(order[j], c).wait_send()

                relay_copy(order[j], c).wait_send()
        for step in range(1, ring):
            go_copy(j, order[j], step).wait_send()
            back_copy(j, order[j], step).wait_send()


def outer_size(size):
    bits = size.bit_length() - 1
    return 1 << -(-bits // 3)


def experts_part(
    normed,
    attended,
    info,
    count,
    ring,
    room,
    weights,
    identity,
):
    length, width = normed.shape
    inside = weights[0].shape[1]
    shared = weights[3].shape[1]
    pieces = 4
    slots = ring * room
    bf16 = jnp.bfloat16
    vmem = pl.BlockSpec(memory_space=pltpu.VMEM)
    anywhere = pl.BlockSpec(memory_space=pl.ANY)
    dma = pltpu.SemaphoreType.DMA
    return pl.pallas_call(
        functools.partial(experts_kernel, count, ring, room, pieces),
        name="experts",
        out_shape=jax.ShapeDtypeStruct((length, width), bf16),
        in_specs=[vmem] * 3 + [anywhere] * 6,
        out_specs=vmem,
        scratch_shapes=[
            pltpu.VMEM((count, length, width), bf16),
            pltpu.VMEM((count,) + info.shape[1:], jnp.float32),
            pltpu.VMEM((count, slots, width), bf16),
            pltpu.VMEM((count, slots, width), bf16),
            pltpu.VMEM((count, slots, width), bf16),
            pltpu.VMEM((count + 1, length, width), bf16),
            pltpu.VMEM((count, length, width), jnp.float32),
            pltpu.VMEM((length, width), jnp.float32),
            pltpu.VMEM((max(slots, length), max(inside, shared)), bf16),
            pltpu.VMEM((slots, length), bf16),
            pltpu.VMEM((2, length, slots), bf16),
        ]
        + [pltpu.VMEM(w.shape, w.dtype) for w in weights]
        + [
            dma((6,)),
            dma((count,)),
            dma((count,)),
            dma((count + 1, pieces)),
            dma((count, pieces)),
            dma((count, ring)),
            dma((count, ring)),
            dma((count, ring)),
            dma((count, ring)),
            dma((count, pieces)),
            dma((count + 1, pieces)),
        ],
        compiler_params=pltpu.CompilerParams(
            collective_id=identity, has_side_effects=True, vmem_limit_bytes=67043328
        ),
    )(normed, attended, info, *weights)


def shards(
    projected_queries,
    projected_keys,
    projected_values,
    output_gate_values,
    write_strength_logits,
    decay_input_logits,
    head_rate_logarithm,
    extra_log_decay,
    per_head_norm_gain,
    output_matrix,
    residual,
    mixture_norm_gain,
    selected_expert_index,
    routing_weight,
    routed_gate_weight,
    routed_up_weight,
    routed_down_weight,
    common_gate_weight,
    common_up_weight,
    common_down_weight,
):
    heads = head_rate_logarithm.shape[0]
    count = outer_size(lax.axis_size("sp"))
    beta = jax.nn.sigmoid(write_strength_logits.astype(jnp.float32))
    decay_logarithm = extra_log_decay - jnp.exp(head_rate_logarithm)[None, :] * jax.nn.softplus(
        decay_input_logits.astype(jnp.float32) - 6.0
    )
    small = jnp.concatenate([beta, decay_logarithm], axis=1)
    small = jnp.pad(small, ((0, 0), (0, 128 - 2 * heads)))
    normed, attended = heads_part(
        projected_queries,
        projected_keys,
        projected_values,
        output_gate_values,
        small,
        per_head_norm_gain[None, :],
        residual,
        mixture_norm_gain[None, :],
        output_matrix,
        heads,
        count,
        0,
    )
    length = normed.shape[0]
    tp_size = lax.axis_size("tp")
    sp_size = lax.axis_size("sp")
    experts = sp_size * tp_size
    ring = experts // count
    room = max(2, length * TOP_K * 3 // (2 * experts))
    room = -(-room // 16) * 16
    chosen = selected_expert_index[:, :, None] == jnp.arange(experts, dtype=jnp.int32)
    named = jnp.any(chosen, axis=1)
    weight = jnp.sum(jnp.where(chosen, routing_weight[:, :, None], 0.0), axis=1)
    place = jnp.arange(length, dtype=jnp.int32)
    earlier = (place[:, None] > place[None, :]).astype(jnp.bfloat16)
    slot = jnp.dot(earlier, named.astype(jnp.bfloat16), preferred_element_type=jnp.float32)
    slot = jnp.where(named, slot, float(room))
    info = jnp.concatenate(
        [slot.T.reshape(count, ring, length), weight.T.reshape(count, ring, length)], axis=1
    )
    weights = (
        routed_gate_weight[0],
        routed_up_weight[0],
        routed_down_weight[0],
        common_gate_weight,
        common_up_weight,
        common_down_weight,
    )
    return experts_part(normed, attended, info, count, ring, room, weights, 2)


def solution(mesh):
    return jax.shard_map(
        shards,
        mesh=mesh,
        in_specs=(
            P("sp", "tp"),
            P("sp", "tp"),
            P("sp", "tp"),
            P("sp", "tp"),
            P("sp", "tp"),
            P("sp", "tp"),
            P("tp"),
            P("sp", "tp"),
            P(),
            P(),
            P(("sp", "tp"), None),
            P(),
            P(("sp", "tp"), None),
            P(("sp", "tp"), None),
            P(("sp", "tp"), None, None),
            P(("sp", "tp"), None, None),
            P(("sp", "tp"), None, None),
            P(),
            P(),
            P(),
        ),
        out_specs=P(("sp", "tp"), None),
        check_vma=False,
    )
```

```python
import functools

import jax
import jax.numpy as jnp
from jax import lax
from jax.experimental import pallas as pl
from jax.experimental.pallas import tpu as pltpu
from jax.sharding import PartitionSpec as P

TOP_K = 4
SPAN = 64
SPLIT = 2
RELAYS = 8


EPS = 1e-06
HIGH = lax.Precision.HIGHEST


def halves(x):
    high = x.astype(jnp.bfloat16)
    return high, (x - high.astype(jnp.float32)).astype(jnp.bfloat16)


NN = (((1,), (0,)), ((), ()))
NT = (((1,), (1,)), ((), ()))


def once(a, b, dims=NN):
    return lax.dot_general(
        a.astype(jnp.bfloat16), b.astype(jnp.bfloat16), dims, preferred_element_type=jnp.float32
    )


def thrice(a, b, dims=NN):
    a_high, a_low = halves(a)
    b_high, b_low = halves(b)

    def dot(x, y):
        return lax.dot_general(x, y, dims, preferred_element_type=jnp.float32)

    return dot(a_high, b_high) + (dot(a_high, b_low) + dot(a_low, b_high))


def silu(x):
    return x * jax.nn.sigmoid(x)


def heads_kernel(
    count,
    span,
    q_ref,
    k_ref,
    v_ref,
    gate_ref,
    small_ref,
    gain_ref,
    residual_ref,
    mixture_gain_ref,
    matrix_hbm,
    normed_ref,
    attended_ref,
    erase,
    fresh,
    score,
    reads,
    late,
    maps,
    fade,
    states,
    changes,
    scale,
    gathered,
    prefix,
    carried,
    starting,
    start,
    mixed,
    finished,
    token_heads,
    matrix,
    matrix_sem,
    ring_send,
    ring_recv,
    line_send,
    line_recv,
    home_send,
    home_recv,
    pair_send,
    pair_recv,
):
    f32 = jnp.float32
    length, columns = q_ref.shape
    heads, number = erase.shape[:2]
    width = columns // heads
    tp_size = lax.axis_size("tp")
    members = lax.axis_size("sp") // count
    parts = members // heads
    slab = width // parts
    sp = lax.axis_index("sp")
    tp = lax.axis_index("tp")
    outer = sp // members
    member = lax.rem(sp, members)
    MESH = pl.DeviceIdType.MESH
    own = length // tp_size

    load = pltpu.make_async_copy(matrix_hbm, matrix, matrix_sem)
    load.start()

    def device(o, m, t):
        return {"sp": o * members + m, "tp": t}

    barrier = pltpu.get_barrier_semaphore()

    def greet(where):
        pl.semaphore_signal(barrier, inc=1, device_id=where, device_id_type=MESH)

    for step in range(1, count):
        greet(device(lax.rem(outer + step, count), member, tp))
    for step in range(1, members):
        greet(device(outer, lax.rem(member + step, members), tp))
    for step in range(1, tp_size):
        greet(device(outer, member, lax.rem(tp + step, tp_size)))

    row = lax.broadcasted_iota(jnp.int32, (span, span), 0)
    column = lax.broadcasted_iota(jnp.int32, (span, span), 1)
    causal = row >= column
    strict = row > column
    one = (row == column).astype(f32)
    lower = causal.astype(f32)
    group = 2 if number % 2 == 0 else 1

    def prepare(it, carry):
        jobs = []
        for part in range(group):
            c = it * group + part
            rows = pl.ds(pl.multiple_of(c * span, span), span)
            small = small_ref[rows, :]
            summed = jnp.dot(
                lower, small, precision=HIGH, preferred_element_type=f32
            )
            turned = summed.T
            for h in range(heads):
                cols = slice(h * width, (h + 1) * width)
                q = silu(q_ref[rows, cols].astype(f32))
                q = q * lax.rsqrt(jnp.sum(q * q, axis=-1, keepdims=True) + EPS)
                k = silu(k_ref[rows, cols].astype(f32))
                k = k * lax.rsqrt(jnp.sum(k * k, axis=-1, keepdims=True) + EPS)
                beta = small[:, h : h + 1]
                g_column = summed[:, heads + h : heads + h + 1]
                g_row = turned[heads + h : heads + h + 1, :]
                decay = jnp.where(
                    causal, jnp.exp(jnp.where(causal, g_column - g_row, 0.0)), 0.0
                )
                kb = k * beta
                both = thrice(jnp.concatenate([kb, q], axis=0), k, NT)
                below = jnp.where(strict, both[:span] * decay, 0.0)
                score[h, c] = both[span:] * decay
                grown = jnp.exp(g_column)
                reads[h, c] = q * grown
                last = g_column[span - 1 :, :]
                late[h, c] = k * jnp.exp(last - g_column)
                fade[h, c] = jnp.broadcast_to(jnp.exp(last), fade.shape[2:])
                v = silu(v_ref[rows, cols].astype(f32)) * beta
                jobs.append((h, c, below, jnp.concatenate([kb * grown, v], axis=1)))
        found = None
        size = 1
        while size < span:
            pair = (row // size) - (column // size)
            mask = ((row // size) % 2 == 1) & (pair == 1)
            pieces = [jnp.where(mask, job[2], 0.0) for job in jobs]
            if found is None:
                found = [one - piece for piece in pieces]
            else:
                inner = [once(x, piece) for x, piece in zip(found, pieces)]
                found = [x - once(y, x) for x, y in zip(found, inner)]
            size *= 2
        wrong = [one - x - thrice(job[2], x) for x, job in zip(found, jobs)]
        found = [x + once(x, e) for x, e in zip(found, wrong)]
        for x, (h, c, _, right) in zip(found, jobs):
            solved = thrice(x, right)
            erase[h, c] = solved[:, :width]
            fresh[h, c] = solved[:, width:].T
        return carry

    lax.fori_loop(0, number // group, prepare, 0)

    square = (
        lax.broadcasted_iota(jnp.int32, (width, width), 0)
        == lax.broadcasted_iota(jnp.int32, (width, width), 1)
    ).astype(f32)
    for h in range(heads):
        maps[h, pl.ds(0, width), :] = square
        maps[h, pl.ds(width, width), :] = jnp.zeros((width, width), f32)

    def advance(c, carry):
        for h in range(heads):
            state = maps[h]
            gone = thrice(state, erase[h, c], NT)
            news = jnp.concatenate([-gone[:width], fresh[h, c] - gone[width:]], axis=0)
            states[h, c] = state
            changes[h, c] = news
            maps[h] = state * fade[h, c, 0:1, :] + thrice(news, late[h, c])
        return carry

    lax.fori_loop(0, number, advance, 0)

    pl.semaphore_wait(barrier, count + members + tp_size - 3)

    def remote(src, dst, send, recv, where):
        return pltpu.make_async_remote_copy(
            src_ref=src,
            dst_ref=dst,
            send_sem=send,
            recv_sem=recv,
            device_id=where,
            device_id_type=MESH,
        )

    def ring_copies(step):
        peer = lax.rem(member + step, members)
        head = peer // parts
        which = lax.rem(peer, parts)
        where = device(outer, peer, tp)
        return (
            remote(
                maps.at[head, pl.ds(0, width)],
                gathered.at[member, pl.ds(0, width)],
                ring_send.at[step, 0],
                ring_recv.at[step, 0],
                where,
            ),
            remote(
                maps.at[head, pl.ds(pl.multiple_of(width + which * slab, slab), slab)],
                gathered.at[member, pl.ds(width, slab)],
                ring_send.at[step, 1],
                ring_recv.at[step, 1],
                where,
            ),
        )

    for step in range(1, members):
        for copy in ring_copies(step):
            copy.start()
    my_head = member // parts
    my_part = lax.rem(member, parts)
    gathered[member, pl.ds(0, width), :] = maps[my_head, pl.ds(0, width), :]
    gathered[member, pl.ds(width, slab), :] = maps[
        my_head, pl.ds(pl.multiple_of(width + my_part * slab, slab), slab), :
    ]

    def local_reads(c, carry):
        rows = pl.ds(pl.multiple_of(c * span, span), span)
        for h in range(heads):
            cols = slice(h * width, (h + 1) * width)
            mixed[h, rows, :] = thrice(reads[h, c], states[h, c], NT) + thrice(
                score[h, c], changes[h, c], NT
            )
            scale[rows, cols] = gain_ref[...] * silu(gate_ref[rows, cols].astype(f32))
        return carry

    lax.fori_loop(0, number, local_reads, 0)
    for step in range(1, members):
        for copy in ring_copies(step):
            copy.wait_recv()

    prefix[0, pl.ds(0, width), :] = square
    prefix[0, pl.ds(width, slab), :] = jnp.zeros((slab, width), f32)
    for r in range(members):
        joined = thrice(prefix[r], gathered[r, pl.ds(0, width), :])
        prefix[r + 1, pl.ds(0, width), :] = joined[:width]
        prefix[r + 1, pl.ds(width, slab), :] = joined[width:] + gathered[r, pl.ds(width, slab), :]

    def line_copy():
        return remote(
            carried.at[1],
            carried.at[0],
            line_send,
            line_recv,
            device(lax.rem(outer + 1, count), member, tp),
        )

    @pl.when(outer == 0)
    def _():
        carried[0] = jnp.zeros((slab, width), f32)

    @pl.when(outer > 0)
    def _():
        line_copy().wait_recv()

    arrived = carried[0]
    carried[1] = (
        thrice(arrived, prefix[members, pl.ds(0, width), :])
        + prefix[members, pl.ds(width, slab), :]
    )

    @pl.when(outer + 1 < count)
    def _():
        line_copy().start()

    for r in range(members):
        starting[r] = (
            thrice(arrived, prefix[r, pl.ds(0, width), :]) + prefix[r, pl.ds(width, slab), :]
        )

    def home_copy(step):
        peer = lax.rem(member + step, members)
        return remote(
            starting.at[peer],
            start.at[my_head, pl.ds(pl.multiple_of(my_part * slab, slab), slab)],
            home_send.at[step],
            home_recv.at[step],
            device(outer, peer, tp),
        )

    def home_landed(step):
        peer = lax.rem(member + members - step, members)
        return remote(
            starting.at[0],
            start.at[peer // parts, pl.ds(pl.multiple_of(lax.rem(peer, parts) * slab, slab), slab)],
            home_send.at[step],
            home_recv.at[step],
            device(outer, lax.rem(member + step, members), tp),
        )

    for step in range(1, members):
        home_copy(step).start()
    start[my_head, pl.ds(pl.multiple_of(my_part * slab, slab), slab), :] = starting[member]
    for step in range(1, members):
        home_landed(step).wait_recv()

    def close(c, carry):
        rows = pl.ds(pl.multiple_of(c * span, span), span)
        for h in range(heads):
            cols = slice(h * width, (h + 1) * width)
            both = mixed[h, rows, :]
            value = both[:, width:] + thrice(both[:, :width], start[h], NT)
            scaled = value * lax.rsqrt(jnp.mean(value * value, axis=-1, keepdims=True) + EPS)
            finished[rows, cols] = (scaled * scale[rows, cols]).astype(jnp.bfloat16)
        return carry

    lax.fori_loop(0, number, close, 0)

    def pair_copy(step):
        peer = lax.rem(tp + step, tp_size)
        return remote(
            finished.at[pl.ds(pl.multiple_of(peer * own, own), own)],
            token_heads.at[tp],
            pair_send.at[step],
            pair_recv.at[step],
            device(outer, member, peer),
        )

    for step in range(1, tp_size):
        pair_copy(step).start()
    token_heads[tp] = finished[pl.ds(pl.multiple_of(tp * own, own), own), :]
    load.wait()
    for step in range(1, tp_size):
        pair_copy(step).wait_recv()

    wide = residual_ref.shape[1]
    tile = min(512, wide)
    squares = jnp.zeros((own, 1), f32)
    for n in range(wide // tile):
        cols = slice(n * tile, (n + 1) * tile)
        value = residual_ref[:, cols].astype(f32)
        for t in range(tp_size):
            value += jnp.dot(
                token_heads[t],
                matrix[pl.ds(t * columns, columns), cols],
                preferred_element_type=f32,
            )
        rounded = value.astype(jnp.bfloat16)
        attended_ref[:, cols] = rounded
        again = rounded.astype(f32)
        squares += jnp.sum(again * again, axis=-1, keepdims=True)
    factor = lax.rsqrt(squares / wide + EPS)
    for n in range(wide // tile):
        cols = slice(n * tile, (n + 1) * tile)
        normed_ref[:, cols] = (
            attended_ref[:, cols].astype(f32) * factor * mixture_gain_ref[:, cols]
        ).astype(jnp.bfloat16)

    for step in range(1, members):
        for copy in ring_copies(step):
            copy.wait_send()
        home_copy(step).wait_send()
    for step in range(1, tp_size):
        pair_copy(step).wait_send()

    @pl.when(outer + 1 < count)
    def _():
        line_copy().wait_send()


def heads_part(
    queries, keys, values, gates, small, gain, residual, mixture_gain, matrix, heads, count, identity
):
    length, columns = queries.shape
    width = columns // heads
    own, wide = residual.shape
    tp_size = lax.axis_size("tp")
    members = lax.axis_size("sp") // count
    parts = members // heads
    slab = width // parts
    span = min(2 * SPAN, length)
    number = length // span
    bf16, f32 = jnp.bfloat16, jnp.float32
    vmem = pl.BlockSpec(memory_space=pltpu.VMEM)
    dma = pltpu.SemaphoreType.DMA
    return pl.pallas_call(
        functools.partial(heads_kernel, count, span),
        name="heads",
        out_shape=[jax.ShapeDtypeStruct((own, wide), bf16)] * 2,
        in_specs=[vmem] * 8 + [pl.BlockSpec(memory_space=pl.ANY)],
        out_specs=[vmem] * 2,
        scratch_shapes=[
            pltpu.VMEM((heads, number, span, width), f32),
            pltpu.VMEM((heads, number, width, span), f32),
            pltpu.VMEM((heads, number, span, span), f32),
            pltpu.VMEM((heads, number, span, width), f32),
            pltpu.VMEM((heads, number, span, width), f32),
            pltpu.VMEM((heads, 2 * width, width), f32),
            pltpu.VMEM((heads, number, 8, width), f32),
            pltpu.VMEM((heads, number, 2 * width, width), f32),
            pltpu.VMEM((heads, number, 2 * width, span), f32),
            pltpu.VMEM((length, columns), f32),
            pltpu.VMEM((members, width + slab, width), f32),
            pltpu.VMEM((members + 1, width + slab, width), f32),
            pltpu.VMEM((2, slab, width), f32),
            pltpu.VMEM((members, slab, width), f32),
            pltpu.VMEM((heads, width, width), f32),
            pltpu.VMEM((heads, length, 2 * width), f32),
            pltpu.VMEM((length, columns), bf16),
            pltpu.VMEM((tp_size, own, columns), bf16),
            pltpu.VMEM(matrix.shape, matrix.dtype),
            dma,
            dma((members, 2)),
            dma((members, 2)),
            dma,
            dma,
            dma((members,)),
            dma((members,)),
            dma((tp_size,)),
            dma((tp_size,)),
        ],
        compiler_params=pltpu.CompilerParams(
            collective_id=identity, has_side_effects=True, vmem_limit_bytes=60000000
        ),
    )(queries, keys, values, gates, small, gain, residual, mixture_gain, matrix)


def lookup(table, index):
    found = table[0]
    for place in range(1, len(table)):
        found = jnp.where(index == place, table[place], found)
    return found


def relay_orders(count):
    arrive, leave, when = [], [], []
    for me in range(count):
        others = [s for s in range(count) if s != me]
        middle = (count - 1) / 2
        arrive.append(sorted(others, key=lambda s: (abs(s - me), abs(s - middle))))

        def key(d):
            reach = (count - 1 - d) if me > d else d
            return (reach, reach - abs(me - d))

        order = sorted(others, key=key)
        leave.append(order)
        steps, latest = [], 0
        for d in order:
            upstream = me + 1 < count if d < me else me > 0
            latest = count - 1 if upstream else max(latest, arrive[me].index(d) + 1)
            steps.append(latest)
        when.append(steps)
    return arrive, leave, when


def experts_kernel(
    count,
    ring,
    room,
    pieces,
    x_ref,
    attended_ref,
    info_ref,
    gate_hbm,
    up_hbm,
    down_hbm,
    common_gate_hbm,
    common_up_hbm,
    common_down_hbm,
    out_ref,
    held,
    tables,
    outbox,
    inbox,
    backbox,
    relay,
    part,
    total,
    hidden,
    picks,
    shares,
    gate,
    up,
    down,
    common_gate,
    common_up,
    common_down,
    weight_sem,
    info_send,
    info_recv,
    hold_send,
    hold_recv,
    go_send,
    go_recv,
    back_send,
    back_recv,
    relay_send,
    relay_recv,
):
    length, width = x_ref.shape
    tp_size = lax.axis_size("tp")
    inner = lax.axis_size("sp") // count
    sp = lax.axis_index("sp")
    outer = sp // inner
    mine = lax.rem(sp, inner) * tp_size + lax.axis_index("tp")
    MESH = pl.DeviceIdType.MESH
    piece = length // pieces
    step_rows = length // RELAYS
    slots = ring * room
    arrive, leave, when = relay_orders(count)

    def device(o, i):
        return {"sp": o * inner + i // tp_size, "tp": lax.rem(i, tp_size)}

    loads = []
    for n, (src, dst) in enumerate(
        (
            (common_gate_hbm, common_gate),
            (common_up_hbm, common_up),
            (common_down_hbm, common_down),
            (gate_hbm, gate),
            (up_hbm, up),
            (down_hbm, down),
        )
    ):
        load = pltpu.make_async_copy(src, dst, weight_sem.at[n])
        load.start()
        loads.append(load)

    barrier = pltpu.get_barrier_semaphore()
    for step in range(1, count):
        pl.semaphore_signal(
            barrier, inc=1, device_id=device(lax.rem(outer + step, count), mine), device_id_type=MESH
        )
    for step in range(1, ring):
        pl.semaphore_signal(
            barrier, inc=1, device_id=device(outer, lax.rem(mine + step, ring)), device_id_type=MESH
        )
    pl.semaphore_wait(barrier, count + ring - 2)

    def remote(src, dst, send, recv, o, i):
        return pltpu.make_async_remote_copy(
            src_ref=src,
            dst_ref=dst,
            send_sem=send,
            recv_sem=recv,
            device_id=device(o, i),
            device_id_type=MESH,
        )

    info_copies = []
    for step in range(1, count):
        peer = lax.rem(outer + step, count)
        copy = remote(
            info_ref.at[peer], tables.at[outer], info_send.at[step], info_recv.at[step], peer, mine
        )
        copy.start()
        info_copies.append(copy)

    def rows_of(c, size):
        return pl.ds(c * size, size)

    has_right = outer + 1 < count
    has_left = outer > 0

    def own_copy(c, right):
        rows = rows_of(c, piece)
        target = outer + 1 if right else outer - 1
        sem = hold_send.at[count, c] if right else hold_send.at[outer, c]
        return remote(x_ref.at[rows], held.at[outer, rows], sem, hold_recv.at[outer, c], target, mine)

    for c in range(pieces):

        @pl.when(has_right)
        def _():
            own_copy(c, True).start()

        @pl.when(has_left)
        def _():
            own_copy(c, False).start()

    held[outer] = x_ref[...]
    tables[outer] = info_ref[outer]

    def matched(source):
        slot = tables[source, :ring, :]
        place = lax.broadcasted_iota(jnp.int32, (ring, room, length), 1).astype(jnp.float32)
        return slot[:, None, :] == place

    def go_copy(j, source, step):
        peer = lax.rem(mine + step, ring)
        rows = pl.ds(pl.multiple_of(peer * room, room), room)
        return remote(
            outbox.at[source, rows],
            inbox.at[source, pl.ds(step * room, room)],
            go_send.at[j, step],
            go_recv.at[j, step],
            outer,
            peer,
        )

    def back_copy(j, source, step):
        peer = lax.rem(mine + ring - step, ring)
        mine_rows = pl.ds(pl.multiple_of(mine * room, room), room)
        return remote(
            inbox.at[source, pl.ds(step * room, room)],
            backbox.at[source, mine_rows],
            back_send.at[j, step],
            back_recv.at[j, step],
            outer,
            peer,
        )

    def spread(j, source):
        picks[...] = (
            jnp.where(matched(source), 1.0, 0.0).reshape(slots, length).astype(jnp.bfloat16)
        )
        tile = min(512, width)

        def body(n, carry):
            cols = pl.ds(pl.multiple_of(n * tile, tile), tile)
            outbox[source, :, cols] = jnp.dot(
                picks[...], held[source, :, cols], preferred_element_type=jnp.float32
            ).astype(jnp.bfloat16)
            return carry

        lax.fori_loop(0, width // tile, body, 0)
        for step in range(1, ring):
            go_copy(j, source, step).start()
        mine_rows = pl.ds(pl.multiple_of(mine * room, room), room)
        inbox[source, pl.ds(0, room), :] = outbox[source, mine_rows, :]

    def feed(rows_ref, count_rows, w_gate, w_up, w_down, store):
        inside = w_gate.shape[1]
        tile = min(256, inside)

        def first(n, carry):
            cols = pl.ds(pl.multiple_of(n * tile, tile), tile)
            rows = rows_ref[...]
            gated = jnp.dot(rows, w_gate[:, cols], preferred_element_type=jnp.float32)
            lifted = jnp.dot(rows, w_up[:, cols], preferred_element_type=jnp.float32)
            hidden[pl.ds(0, count_rows), cols] = (gated * jax.nn.sigmoid(gated) * lifted).astype(
                jnp.bfloat16
            )
            return carry

        lax.fori_loop(0, inside // tile, first, 0)
        wide = min(512, width)

        def second(n, carry):
            cols = pl.ds(pl.multiple_of(n * wide, wide), wide)
            store(
                cols,
                jnp.dot(
                    hidden[pl.ds(0, count_rows), :],
                    w_down[:, cols],
                    preferred_element_type=jnp.float32,
                ),
            )
            return carry

        lax.fori_loop(0, width // wide, second, 0)

    def serve(j, source, returns):
        for part in range(SPLIT):
            steps = range(part * ring // SPLIT, (part + 1) * ring // SPLIT)
            rows = pl.ds(steps[0] * room, len(steps) * room)
            for step in steps:
                if step > 0:
                    go_copy(j, source, step).wait_recv()

            def store(cols, value):
                inbox[source, rows, cols] = value.astype(jnp.bfloat16)

            feed(inbox.at[source, rows], len(steps) * room, gate, up, down, store)
            if returns:
                send_back(j, source, steps)

    def send_back(j, source, steps):
        for step in steps:
            if step > 0:
                back_copy(j, source, step).start()
            else:
                mine_rows = pl.ds(pl.multiple_of(mine * room, room), room)
                backbox[source, mine_rows, :] = inbox[source, pl.ds(0, room), :]

    def combine(j, source, store):
        weight = tables[source, ring:, :]
        spread_weight = jnp.where(matched(source), weight[:, None, :], 0.0).reshape(slots, length)
        turned = spread_weight.T
        high = turned.astype(jnp.bfloat16)
        shares[0] = high
        shares[1] = (turned - high.astype(jnp.float32)).astype(jnp.bfloat16)
        for step in range(1, ring):
            back_copy(j, source, step).wait_recv()
        tile = min(512, width)

        def body(n, carry):
            cols = pl.ds(pl.multiple_of(n * tile, tile), tile)
            rows = backbox[source, :, cols]
            store(
                cols,
                jnp.dot(shares[0], rows, preferred_element_type=jnp.float32)
                + jnp.dot(shares[1], rows, preferred_element_type=jnp.float32),
            )
            return carry

        lax.fori_loop(0, width // tile, body, 0)

    def forward_copy(source, c):
        rows = rows_of(c, piece)
        target = jnp.where(source < outer, outer + 1, outer - 1)
        return remote(
            held.at[source, rows],
            held.at[source, rows],
            hold_send.at[jnp.where(source < outer, source, source), c],
            hold_recv.at[source, c],
            target,
            mine,
        )

    def goes_on(source):
        return ((source < outer) & has_right) | ((source > outer) & has_left)

    def receive(source):
        for c in range(pieces):
            forward_copy(source, c).wait_recv()

            @pl.when(goes_on(source))
            def _():
                forward_copy(source, c).start()

    def relay_copy(dest, c):
        rows = rows_of(c, step_rows)
        leftward = dest < outer
        target = jnp.where(leftward, outer - 1, outer + 1)
        landing = jnp.where(leftward & (target == dest), count, dest)
        return remote(
            relay.at[dest, rows],
            relay.at[landing, rows],
            relay_send.at[dest, c],
            relay_recv.at[landing, c],
            target,
            mine,
        )

    def landed(place, c):
        rows = rows_of(c, step_rows)
        return remote(
            relay.at[place, rows],
            relay.at[place, rows],
            relay_send.at[0, c],
            relay_recv.at[place, c],
            lax.rem(outer + 1, count),
            mine,
        )

    def pass_on(dest):
        upstream = ((dest < outer) & has_right) | ((dest > outer) & has_left)
        for c in range(RELAYS):
            rows = rows_of(c, step_rows)

            @pl.when(upstream)
            def _():
                landed(dest, c).wait_recv()
                relay[dest, rows, :] = (
                    relay[dest, rows, :].astype(jnp.float32) + part[dest, rows, :]
                ).astype(jnp.bfloat16)

            @pl.when(jnp.logical_not(upstream))
            def _():
                relay[dest, rows, :] = part[dest, rows, :].astype(jnp.bfloat16)

            relay_copy(dest, c).start()

    order = [outer] + [lookup([arrive[m][j] for m in range(count)], outer) for j in range(count - 1)]
    drain = [lookup([leave[m][j] for m in range(count)], outer) for j in range(count - 1)]

    spread(0, outer)
    for load in loads[:3]:
        load.wait()

    def keep(cols, value):
        total[:, cols] = attended_ref[:, cols].astype(jnp.float32) + value

    feed(x_ref, length, common_gate, common_up, common_down, keep)
    for copy in info_copies:
        copy.wait_recv()

    def store_part(source):
        def store(cols, value):
            part[source, :, cols] = value

        return store

    def collect(j):
        combine(j, order[j], store_part(order[j]))
        for k in range(count - 1):
            places = [when[m][k] for m in range(count)]
            if j in places:
                if all(p == j for p in places):
                    pass_on(drain[k])
                else:

                    @pl.when(lookup([int(p == j) for p in places], outer) == 1)
                    def _():
                        pass_on(drain[k])

    last = count - 1
    between = has_left & has_right
    at_end = jnp.logical_not(between)

    def early(j):
        if j <= last:

            @pl.when(between)
            def _():
                receive(order[j])

    def late_receive(j):
        @pl.when(at_end)
        def _():
            receive(order[j])

    receive(order[1])
    spread(1, order[1])
    early(2)
    for load in loads[3:]:
        load.wait()
    serve(0, order[0], False)
    for j in range(1, last):
        if j == 1:
            serve(j, order[j], True)
        early(j + 2)
        late_receive(j + 1)
        spread(j + 1, order[j + 1])
        if j < last - 1:
            collect(j)
        if j > 1:
            serve(j, order[j], True)
    serve(last, order[last], True)
    send_back(0, order[0], range(ring))
    if last > 1:
        collect(last - 1)
    collect(last)

    def add(cols, value):
        total[:, cols] += value

    combine(0, order[0], add)
    for side, place in ((has_left, outer), (has_right, count)):
        for c in range(RELAYS):
            rows = rows_of(c, step_rows)

            @pl.when(side)
            def _():
                landed(place, c).wait_recv()
                total[rows, :] += relay[place, rows, :].astype(jnp.float32)

    out_ref[...] = total[...].astype(jnp.bfloat16)

    for copy in info_copies:
        copy.wait_send()
    for c in range(pieces):

        @pl.when(has_right)
        def _():
            own_copy(c, True).wait_send()

        @pl.when(has_left)
        def _():
            own_copy(c, False).wait_send()

    for j in range(count):
        if j > 0:
            for c in range(pieces):

                @pl.when(goes_on(order[j]))
                def _():
                    forward_copy(order[j], c).wait_send()

            for c in range(RELAYS):
                relay_copy(order[j], c).wait_send()
        for step in range(1, ring):
            go_copy(j, order[j], step).wait_send()
            back_copy(j, order[j], step).wait_send()


def outer_size(size):
    bits = size.bit_length() - 1
    return 1 << -(-bits // 3)


def experts_part(
    normed,
    attended,
    info,
    count,
    ring,
    room,
    weights,
    identity,
):
    length, width = normed.shape
    inside = weights[0].shape[1]
    shared = weights[3].shape[1]
    pieces = 4
    slots = ring * room
    bf16 = jnp.bfloat16
    vmem = pl.BlockSpec(memory_space=pltpu.VMEM)
    anywhere = pl.BlockSpec(memory_space=pl.ANY)
    dma = pltpu.SemaphoreType.DMA
    return pl.pallas_call(
        functools.partial(experts_kernel, count, ring, room, pieces),
        name="experts",
        out_shape=jax.ShapeDtypeStruct((length, width), bf16),
        in_specs=[vmem] * 3 + [anywhere] * 6,
        out_specs=vmem,
        scratch_shapes=[
            pltpu.VMEM((count, length, width), bf16),
            pltpu.VMEM((count,) + info.shape[1:], jnp.float32),
            pltpu.VMEM((count, slots, width), bf16),
            pltpu.VMEM((count, slots, width), bf16),
            pltpu.VMEM((count, slots, width), bf16),
            pltpu.VMEM((count + 1, length, width), bf16),
            pltpu.VMEM((count, length, width), jnp.float32),
            pltpu.VMEM((length, width), jnp.float32),
            pltpu.VMEM((max(slots, length), max(inside, shared)), bf16),
            pltpu.VMEM((slots, length), bf16),
            pltpu.VMEM((2, length, slots), bf16),
        ]
        + [pltpu.VMEM(w.shape, w.dtype) for w in weights]
        + [
            dma((6,)),
            dma((count,)),
            dma((count,)),
            dma((count + 1, pieces)),
            dma((count, pieces)),
            dma((count, ring)),
            dma((count, ring)),
            dma((count, ring)),
            dma((count, ring)),
            dma((count, RELAYS)),
            dma((count + 1, RELAYS)),
        ],
        compiler_params=pltpu.CompilerParams(
            collective_id=identity, has_side_effects=True, vmem_limit_bytes=67043328
        ),
    )(normed, attended, info, *weights)


def shards(
    projected_queries,
    projected_keys,
    projected_values,
    output_gate_values,
    write_strength_logits,
    decay_input_logits,
    head_rate_logarithm,
    extra_log_decay,
    per_head_norm_gain,
    output_matrix,
    residual,
    mixture_norm_gain,
    selected_expert_index,
    routing_weight,
    routed_gate_weight,
    routed_up_weight,
    routed_down_weight,
    common_gate_weight,
    common_up_weight,
    common_down_weight,
):
    heads = head_rate_logarithm.shape[0]
    count = outer_size(lax.axis_size("sp"))
    beta = jax.nn.sigmoid(write_strength_logits.astype(jnp.float32))
    decay_logarithm = extra_log_decay - jnp.exp(head_rate_logarithm)[None, :] * jax.nn.softplus(
        decay_input_logits.astype(jnp.float32) - 6.0
    )
    small = jnp.concatenate([beta, decay_logarithm], axis=1)
    small = jnp.pad(small, ((0, 0), (0, 128 - 2 * heads)))
    normed, attended = heads_part(
        projected_queries,
        projected_keys,
        projected_values,
        output_gate_values,
        small,
        per_head_norm_gain[None, :],
        residual,
        mixture_norm_gain[None, :],
        output_matrix,
        heads,
        count,
        0,
    )
    length = normed.shape[0]
    tp_size = lax.axis_size("tp")
    sp_size = lax.axis_size("sp")
    experts = sp_size * tp_size
    ring = experts // count
    room = max(2, length * TOP_K * 3 // (2 * experts))
    room = -(-room // 16) * 16
    chosen = selected_expert_index[:, :, None] == jnp.arange(experts, dtype=jnp.int32)
    named = jnp.any(chosen, axis=1)
    weight = jnp.sum(jnp.where(chosen, routing_weight[:, :, None], 0.0), axis=1)
    place = jnp.arange(length, dtype=jnp.int32)
    earlier = (place[:, None] > place[None, :]).astype(jnp.bfloat16)
    slot = jnp.dot(earlier, named.astype(jnp.bfloat16), preferred_element_type=jnp.float32)
    slot = jnp.where(named, slot, float(room))
    info = jnp.concatenate(
        [slot.T.reshape(count, ring, length), weight.T.reshape(count, ring, length)], axis=1
    )
    weights = (
        routed_gate_weight[0],
        routed_up_weight[0],
        routed_down_weight[0],
        common_gate_weight,
        common_up_weight,
        common_down_weight,
    )
    return experts_part(normed, attended, info, count, ring, room, weights, 2)


def solution(mesh):
    return jax.shard_map(
        shards,
        mesh=mesh,
        in_specs=(
            P("sp", "tp"),
            P("sp", "tp"),
            P("sp", "tp"),
            P("sp", "tp"),
            P("sp", "tp"),
            P("sp", "tp"),
            P("tp"),
            P("sp", "tp"),
            P(),
            P(),
            P(("sp", "tp"), None),
            P(),
            P(("sp", "tp"), None),
            P(("sp", "tp"), None),
            P(("sp", "tp"), None, None),
            P(("sp", "tp"), None, None),
            P(("sp", "tp"), None, None),
            P(),
            P(),
            P(),
        ),
        out_specs=P(("sp", "tp"), None),
        check_vma=False,
    )
```

```python
import functools

import jax
import jax.numpy as jnp
from jax import lax
from jax.experimental import pallas as pl
from jax.experimental.pallas import tpu as pltpu
from jax.sharding import PartitionSpec as P

TOP_K = 4
SPAN = 64
SPLIT = 2
RELAYS = 8


EPS = 1e-06
HIGH = lax.Precision.HIGHEST


def halves(x):
    high = x.astype(jnp.bfloat16)
    return high, (x - high.astype(jnp.float32)).astype(jnp.bfloat16)


NN = (((1,), (0,)), ((), ()))
NT = (((1,), (1,)), ((), ()))


def once(a, b, dims=NN):
    return lax.dot_general(
        a.astype(jnp.bfloat16), b.astype(jnp.bfloat16), dims, preferred_element_type=jnp.float32
    )


def thrice(a, b, dims=NN):
    a_high, a_low = halves(a)
    b_high, b_low = halves(b)

    def dot(x, y):
        return lax.dot_general(x, y, dims, preferred_element_type=jnp.float32)

    return dot(a_high, b_high) + (dot(a_high, b_low) + dot(a_low, b_high))


def silu(x):
    return x * jax.nn.sigmoid(x)


def heads_kernel(
    count,
    span,
    q_ref,
    k_ref,
    v_ref,
    gate_ref,
    small_ref,
    gain_ref,
    residual_ref,
    mixture_gain_ref,
    matrix_hbm,
    normed_ref,
    attended_ref,
    erase,
    fresh,
    score,
    reads,
    late,
    maps,
    fade,
    states,
    changes,
    scale,
    gathered,
    prefix,
    carried,
    starting,
    start,
    mixed,
    finished,
    token_heads,
    matrix,
    matrix_sem,
    ring_send,
    ring_recv,
    line_send,
    line_recv,
    home_send,
    home_recv,
    pair_send,
    pair_recv,
):
    f32 = jnp.float32
    length, columns = q_ref.shape
    heads, number = erase.shape[:2]
    width = columns // heads
    tp_size = lax.axis_size("tp")
    members = lax.axis_size("sp") // count
    parts = members // heads
    slab = width // parts
    sp = lax.axis_index("sp")
    tp = lax.axis_index("tp")
    outer = sp // members
    member = lax.rem(sp, members)
    MESH = pl.DeviceIdType.MESH
    own = length // tp_size

    load = pltpu.make_async_copy(matrix_hbm, matrix, matrix_sem)
    load.start()

    def device(o, m, t):
        return {"sp": o * members + m, "tp": t}

    barrier = pltpu.get_barrier_semaphore()

    def greet(where):
        pl.semaphore_signal(barrier, inc=1, device_id=where, device_id_type=MESH)

    for step in range(1, count):
        greet(device(lax.rem(outer + step, count), member, tp))
    for step in range(1, members):
        greet(device(outer, lax.rem(member + step, members), tp))
    for step in range(1, tp_size):
        greet(device(outer, member, lax.rem(tp + step, tp_size)))

    row = lax.broadcasted_iota(jnp.int32, (span, span), 0)
    column = lax.broadcasted_iota(jnp.int32, (span, span), 1)
    causal = row >= column
    strict = row > column
    one = (row == column).astype(f32)
    lower = causal.astype(f32)
    group = 2 if number % 2 == 0 else 1

    def prepare(it, carry):
        jobs = []
        for part in range(group):
            c = it * group + part
            rows = pl.ds(pl.multiple_of(c * span, span), span)
            small = small_ref[rows, :]
            summed = jnp.dot(
                lower, small, precision=HIGH, preferred_element_type=f32
            )
            turned = summed.T
            for h in range(heads):
                cols = slice(h * width, (h + 1) * width)
                q = silu(q_ref[rows, cols].astype(f32))
                q = q * lax.rsqrt(jnp.sum(q * q, axis=-1, keepdims=True) + EPS)
                k = silu(k_ref[rows, cols].astype(f32))
                k = k * lax.rsqrt(jnp.sum(k * k, axis=-1, keepdims=True) + EPS)
                beta = small[:, h : h + 1]
                g_column = summed[:, heads + h : heads + h + 1]
                g_row = turned[heads + h : heads + h + 1, :]
                decay = jnp.where(
                    causal, jnp.exp(jnp.where(causal, g_column - g_row, 0.0)), 0.0
                )
                kb = k * beta
                both = once(jnp.concatenate([kb, q], axis=0), k, NT)
                below = jnp.where(strict, both[:span] * decay, 0.0)
                score[h, c] = both[span:] * decay
                grown = jnp.exp(g_column)
                reads[h, c] = q * grown
                last = g_column[span - 1 :, :]
                late[h, c] = k * jnp.exp(last - g_column)
                fade[h, c] = jnp.broadcast_to(jnp.exp(last), fade.shape[2:])
                v = silu(v_ref[rows, cols].astype(f32)) * beta
                jobs.append((h, c, below, jnp.concatenate([kb * grown, v], axis=1)))
        found = None
        size = 1
        while size < span:
            pair = (row // size) - (column // size)
            mask = ((row // size) % 2 == 1) & (pair == 1)
            pieces = [jnp.where(mask, job[2], 0.0) for job in jobs]
            if found is None:
                found = [one - piece for piece in pieces]
            else:
                inner = [once(x, piece) for x, piece in zip(found, pieces)]
                found = [x - once(y, x) for x, y in zip(found, inner)]
            size *= 2
        wrong = [one - x - thrice(job[2], x) for x, job in zip(found, jobs)]
        found = [x + once(x, e) for x, e in zip(found, wrong)]
        for x, (h, c, _, right) in zip(found, jobs):
            solved = thrice(x, right)
            erase[h, c] = solved[:, :width]
            fresh[h, c] = solved[:, width:].T
        return carry

    lax.fori_loop(0, number // group, prepare, 0)

    square = (
        lax.broadcasted_iota(jnp.int32, (width, width), 0)
        == lax.broadcasted_iota(jnp.int32, (width, width), 1)
    ).astype(f32)
    for h in range(heads):
        maps[h, pl.ds(0, width), :] = square
        maps[h, pl.ds(width, width), :] = jnp.zeros((width, width), f32)

    def advance(c, carry):
        for h in range(heads):
            state = maps[h]
            gone = thrice(state, erase[h, c], NT)
            news = jnp.concatenate([-gone[:width], fresh[h, c] - gone[width:]], axis=0)
            states[h, c] = state
            changes[h, c] = news
            maps[h] = state * fade[h, c, 0:1, :] + thrice(news, late[h, c])
        return carry

    lax.fori_loop(0, number, advance, 0)

    pl.semaphore_wait(barrier, count + members + tp_size - 3)

    def remote(src, dst, send, recv, where):
        return pltpu.make_async_remote_copy(
            src_ref=src,
            dst_ref=dst,
            send_sem=send,
            recv_sem=recv,
            device_id=where,
            device_id_type=MESH,
        )

    def ring_copies(step):
        peer = lax.rem(member + step, members)
        head = peer // parts
        which = lax.rem(peer, parts)
        where = device(outer, peer, tp)
        return (
            remote(
                maps.at[head, pl.ds(0, width)],
                gathered.at[member, pl.ds(0, width)],
                ring_send.at[step, 0],
                ring_recv.at[step, 0],
                where,
            ),
            remote(
                maps.at[head, pl.ds(pl.multiple_of(width + which * slab, slab), slab)],
                gathered.at[member, pl.ds(width, slab)],
                ring_send.at[step, 1],
                ring_recv.at[step, 1],
                where,
            ),
        )

    for step in range(1, members):
        for copy in ring_copies(step):
            copy.start()
    my_head = member // parts
    my_part = lax.rem(member, parts)
    gathered[member, pl.ds(0, width), :] = maps[my_head, pl.ds(0, width), :]
    gathered[member, pl.ds(width, slab), :] = maps[
        my_head, pl.ds(pl.multiple_of(width + my_part * slab, slab), slab), :
    ]

    def local_reads(c, carry):
        rows = pl.ds(pl.multiple_of(c * span, span), span)
        for h in range(heads):
            cols = slice(h * width, (h + 1) * width)
            mixed[h, rows, :] = once(reads[h, c], states[h, c], NT) + once(
                score[h, c], changes[h, c], NT
            )
            scale[rows, cols] = gain_ref[...] * silu(gate_ref[rows, cols].astype(f32))
        return carry

    lax.fori_loop(0, number, local_reads, 0)
    for step in range(1, members):
        for copy in ring_copies(step):
            copy.wait_recv()

    prefix[0, pl.ds(0, width), :] = square
    prefix[0, pl.ds(width, slab), :] = jnp.zeros((slab, width), f32)
    for r in range(members):
        joined = thrice(prefix[r], gathered[r, pl.ds(0, width), :])
        prefix[r + 1, pl.ds(0, width), :] = joined[:width]
        prefix[r + 1, pl.ds(width, slab), :] = joined[width:] + gathered[r, pl.ds(width, slab), :]

    def line_copy():
        return remote(
            carried.at[1],
            carried.at[0],
            line_send,
            line_recv,
            device(lax.rem(outer + 1, count), member, tp),
        )

    @pl.when(outer == 0)
    def _():
        carried[0] = jnp.zeros((slab, width), f32)

    @pl.when(outer > 0)
    def _():
        line_copy().wait_recv()

    arrived = carried[0]
    carried[1] = (
        thrice(arrived, prefix[members, pl.ds(0, width), :])
        + prefix[members, pl.ds(width, slab), :]
    )

    @pl.when(outer + 1 < count)
    def _():
        line_copy().start()

    for r in range(members):
        starting[r] = (
            thrice(arrived, prefix[r, pl.ds(0, width), :]) + prefix[r, pl.ds(width, slab), :]
        )

    def home_copy(step):
        peer = lax.rem(member + step, members)
        return remote(
            starting.at[peer],
            start.at[my_head, pl.ds(pl.multiple_of(my_part * slab, slab), slab)],
            home_send.at[step],
            home_recv.at[step],
            device(outer, peer, tp),
        )

    def home_landed(step):
        peer = lax.rem(member + members - step, members)
        return remote(
            starting.at[0],
            start.at[peer // parts, pl.ds(pl.multiple_of(lax.rem(peer, parts) * slab, slab), slab)],
            home_send.at[step],
            home_recv.at[step],
            device(outer, lax.rem(member + step, members), tp),
        )

    for step in range(1, members):
        home_copy(step).start()
    start[my_head, pl.ds(pl.multiple_of(my_part * slab, slab), slab), :] = starting[member]
    for step in range(1, members):
        home_landed(step).wait_recv()

    def close(c, carry):
        rows = pl.ds(pl.multiple_of(c * span, span), span)
        for h in range(heads):
            cols = slice(h * width, (h + 1) * width)
            both = mixed[h, rows, :]
            value = both[:, width:] + thrice(both[:, :width], start[h], NT)
            scaled = value * lax.rsqrt(jnp.mean(value * value, axis=-1, keepdims=True) + EPS)
            finished[rows, cols] = (scaled * scale[rows, cols]).astype(jnp.bfloat16)
        return carry

    lax.fori_loop(0, number, close, 0)

    def pair_copy(step):
        peer = lax.rem(tp + step, tp_size)
        return remote(
            finished.at[pl.ds(pl.multiple_of(peer * own, own), own)],
            token_heads.at[tp],
            pair_send.at[step],
            pair_recv.at[step],
            device(outer, member, peer),
        )

    for step in range(1, tp_size):
        pair_copy(step).start()
    token_heads[tp] = finished[pl.ds(pl.multiple_of(tp * own, own), own), :]
    load.wait()
    for step in range(1, tp_size):
        pair_copy(step).wait_recv()

    wide = residual_ref.shape[1]
    tile = min(512, wide)
    squares = jnp.zeros((own, 1), f32)
    for n in range(wide // tile):
        cols = slice(n * tile, (n + 1) * tile)
        value = residual_ref[:, cols].astype(f32)
        for t in range(tp_size):
            value += jnp.dot(
                token_heads[t],
                matrix[pl.ds(t * columns, columns), cols],
                preferred_element_type=f32,
            )
        rounded = value.astype(jnp.bfloat16)
        attended_ref[:, cols] = rounded
        again = rounded.astype(f32)
        squares += jnp.sum(again * again, axis=-1, keepdims=True)
    factor = lax.rsqrt(squares / wide + EPS)
    for n in range(wide // tile):
        cols = slice(n * tile, (n + 1) * tile)
        normed_ref[:, cols] = (
            attended_ref[:, cols].astype(f32) * factor * mixture_gain_ref[:, cols]
        ).astype(jnp.bfloat16)

    for step in range(1, members):
        for copy in ring_copies(step):
            copy.wait_send()
        home_copy(step).wait_send()
    for step in range(1, tp_size):
        pair_copy(step).wait_send()

    @pl.when(outer + 1 < count)
    def _():
        line_copy().wait_send()


def heads_part(
    queries, keys, values, gates, small, gain, residual, mixture_gain, matrix, heads, count, identity
):
    length, columns = queries.shape
    width = columns // heads
    own, wide = residual.shape
    tp_size = lax.axis_size("tp")
    members = lax.axis_size("sp") // count
    parts = members // heads
    slab = width // parts
    span = min(2 * SPAN, length)
    number = length // span
    bf16, f32 = jnp.bfloat16, jnp.float32
    vmem = pl.BlockSpec(memory_space=pltpu.VMEM)
    dma = pltpu.SemaphoreType.DMA
    return pl.pallas_call(
        functools.partial(heads_kernel, count, span),
        name="heads",
        out_shape=[jax.ShapeDtypeStruct((own, wide), bf16)] * 2,
        in_specs=[vmem] * 8 + [pl.BlockSpec(memory_space=pl.ANY)],
        out_specs=[vmem] * 2,
        scratch_shapes=[
            pltpu.VMEM((heads, number, span, width), f32),
            pltpu.VMEM((heads, number, width, span), f32),
            pltpu.VMEM((heads, number, span, span), f32),
            pltpu.VMEM((heads, number, span, width), f32),
            pltpu.VMEM((heads, number, span, width), f32),
            pltpu.VMEM((heads, 2 * width, width), f32),
            pltpu.VMEM((heads, number, 8, width), f32),
            pltpu.VMEM((heads, number, 2 * width, width), f32),
            pltpu.VMEM((heads, number, 2 * width, span), f32),
            pltpu.VMEM((length, columns), f32),
            pltpu.VMEM((members, width + slab, width), f32),
            pltpu.VMEM((members + 1, width + slab, width), f32),
            pltpu.VMEM((2, slab, width), f32),
            pltpu.VMEM((members, slab, width), f32),
            pltpu.VMEM((heads, width, width), f32),
            pltpu.VMEM((heads, length, 2 * width), f32),
            pltpu.VMEM((length, columns), bf16),
            pltpu.VMEM((tp_size, own, columns), bf16),
            pltpu.VMEM(matrix.shape, matrix.dtype),
            dma,
            dma((members, 2)),
            dma((members, 2)),
            dma,
            dma,
            dma((members,)),
            dma((members,)),
            dma((tp_size,)),
            dma((tp_size,)),
        ],
        compiler_params=pltpu.CompilerParams(
            collective_id=identity, has_side_effects=True, vmem_limit_bytes=60000000
        ),
    )(queries, keys, values, gates, small, gain, residual, mixture_gain, matrix)


def lookup(table, index):
    found = table[0]
    for place in range(1, len(table)):
        found = jnp.where(index == place, table[place], found)
    return found


def relay_orders(count):
    arrive, leave, when = [], [], []
    for me in range(count):
        others = [s for s in range(count) if s != me]
        middle = (count - 1) / 2
        arrive.append(sorted(others, key=lambda s: (abs(s - me), abs(s - middle))))

        def key(d):
            reach = (count - 1 - d) if me > d else d
            return (reach, reach - abs(me - d))

        order = sorted(others, key=key)
        leave.append(order)
        steps, latest = [], 0
        for d in order:
            upstream = me + 1 < count if d < me else me > 0
            latest = count - 1 if upstream else max(latest, arrive[me].index(d) + 1)
            steps.append(latest)
        when.append(steps)
    return arrive, leave, when


def experts_kernel(
    count,
    ring,
    room,
    pieces,
    x_ref,
    attended_ref,
    info_ref,
    gate_hbm,
    up_hbm,
    down_hbm,
    common_gate_hbm,
    common_up_hbm,
    common_down_hbm,
    out_ref,
    held,
    tables,
    outbox,
    inbox,
    backbox,
    relay,
    part,
    total,
    hidden,
    picks,
    shares,
    gate,
    up,
    down,
    common_gate,
    common_up,
    common_down,
    weight_sem,
    info_send,
    info_recv,
    hold_send,
    hold_recv,
    go_send,
    go_recv,
    back_send,
    back_recv,
    relay_send,
    relay_recv,
):
    length, width = x_ref.shape
    tp_size = lax.axis_size("tp")
    inner = lax.axis_size("sp") // count
    sp = lax.axis_index("sp")
    outer = sp // inner
    mine = lax.rem(sp, inner) * tp_size + lax.axis_index("tp")
    MESH = pl.DeviceIdType.MESH
    piece = length // pieces
    step_rows = length // RELAYS
    slots = ring * room
    arrive, leave, when = relay_orders(count)

    def device(o, i):
        return {"sp": o * inner + i // tp_size, "tp": lax.rem(i, tp_size)}

    loads = []
    for n, (src, dst) in enumerate(
        (
            (common_gate_hbm, common_gate),
            (common_up_hbm, common_up),
            (common_down_hbm, common_down),
            (gate_hbm, gate),
            (up_hbm, up),
            (down_hbm, down),
        )
    ):
        load = pltpu.make_async_copy(src, dst, weight_sem.at[n])
        load.start()
        loads.append(load)

    barrier = pltpu.get_barrier_semaphore()
    for step in range(1, count):
        pl.semaphore_signal(
            barrier, inc=1, device_id=device(lax.rem(outer + step, count), mine), device_id_type=MESH
        )
    for step in range(1, ring):
        pl.semaphore_signal(
            barrier, inc=1, device_id=device(outer, lax.rem(mine + step, ring)), device_id_type=MESH
        )
    pl.semaphore_wait(barrier, count + ring - 2)

    def remote(src, dst, send, recv, o, i):
        return pltpu.make_async_remote_copy(
            src_ref=src,
            dst_ref=dst,
            send_sem=send,
            recv_sem=recv,
            device_id=device(o, i),
            device_id_type=MESH,
        )

    info_copies = []
    for step in range(1, count):
        peer = lax.rem(outer + step, count)
        copy = remote(
            info_ref.at[peer], tables.at[outer], info_send.at[step], info_recv.at[step], peer, mine
        )
        copy.start()
        info_copies.append(copy)

    def rows_of(c, size):
        return pl.ds(c * size, size)

    has_right = outer + 1 < count
    has_left = outer > 0

    def own_copy(c, right):
        rows = rows_of(c, piece)
        target = outer + 1 if right else outer - 1
        sem = hold_send.at[count, c] if right else hold_send.at[outer, c]
        return remote(x_ref.at[rows], held.at[outer, rows], sem, hold_recv.at[outer, c], target, mine)

    for c in range(pieces):

        @pl.when(has_right)
        def _():
            own_copy(c, True).start()

        @pl.when(has_left)
        def _():
            own_copy(c, False).start()

    held[outer] = x_ref[...]
    tables[outer] = info_ref[outer]

    def matched(source):
        slot = tables[source, :ring, :]
        place = lax.broadcasted_iota(jnp.int32, (ring, room, length), 1).astype(jnp.float32)
        return slot[:, None, :] == place

    def go_copy(j, source, step):
        peer = lax.rem(mine + step, ring)
        rows = pl.ds(pl.multiple_of(peer * room, room), room)
        return remote(
            outbox.at[source, rows],
            inbox.at[source, pl.ds(step * room, room)],
            go_send.at[j, step],
            go_recv.at[j, step],
            outer,
            peer,
        )

    def back_copy(j, source, step):
        peer = lax.rem(mine + ring - step, ring)
        mine_rows = pl.ds(pl.multiple_of(mine * room, room), room)
        return remote(
            inbox.at[source, pl.ds(step * room, room)],
            backbox.at[source, mine_rows],
            back_send.at[j, step],
            back_recv.at[j, step],
            outer,
            peer,
        )

    def spread(j, source):
        picks[...] = (
            jnp.where(matched(source), 1.0, 0.0).reshape(slots, length).astype(jnp.bfloat16)
        )
        tile = min(512, width)

        def body(n, carry):
            cols = pl.ds(pl.multiple_of(n * tile, tile), tile)
            outbox[source, :, cols] = jnp.dot(
                picks[...], held[source, :, cols], preferred_element_type=jnp.float32
            ).astype(jnp.bfloat16)
            return carry

        lax.fori_loop(0, width // tile, body, 0)
        for step in range(1, ring):
            go_copy(j, source, step).start()
        mine_rows = pl.ds(pl.multiple_of(mine * room, room), room)
        inbox[source, pl.ds(0, room), :] = outbox[source, mine_rows, :]

    def feed(rows_ref, count_rows, w_gate, w_up, w_down, store):
        inside = w_gate.shape[1]
        tile = min(256, inside)

        def first(n, carry):
            cols = pl.ds(pl.multiple_of(n * tile, tile), tile)
            rows = rows_ref[...]
            gated = jnp.dot(rows, w_gate[:, cols], preferred_element_type=jnp.float32)
            lifted = jnp.dot(rows, w_up[:, cols], preferred_element_type=jnp.float32)
            hidden[pl.ds(0, count_rows), cols] = (gated * jax.nn.sigmoid(gated) * lifted).astype(
                jnp.bfloat16
            )
            return carry

        lax.fori_loop(0, inside // tile, first, 0)
        wide = min(512, width)

        def second(n, carry):
            cols = pl.ds(pl.multiple_of(n * wide, wide), wide)
            store(
                cols,
                jnp.dot(
                    hidden[pl.ds(0, count_rows), :],
                    w_down[:, cols],
                    preferred_element_type=jnp.float32,
                ),
            )
            return carry

        lax.fori_loop(0, width // wide, second, 0)

    def serve(j, source, returns):
        for part in range(SPLIT):
            steps = range(part * ring // SPLIT, (part + 1) * ring // SPLIT)
            rows = pl.ds(steps[0] * room, len(steps) * room)
            for step in steps:
                if step > 0:
                    go_copy(j, source, step).wait_recv()

            def store(cols, value):
                inbox[source, rows, cols] = value.astype(jnp.bfloat16)

            feed(inbox.at[source, rows], len(steps) * room, gate, up, down, store)
            if returns:
                send_back(j, source, steps)

    def send_back(j, source, steps):
        for step in steps:
            if step > 0:
                back_copy(j, source, step).start()
            else:
                mine_rows = pl.ds(pl.multiple_of(mine * room, room), room)
                backbox[source, mine_rows, :] = inbox[source, pl.ds(0, room), :]

    def combine(j, source, store):
        weight = tables[source, ring:, :]
        spread_weight = jnp.where(matched(source), weight[:, None, :], 0.0).reshape(slots, length)
        turned = spread_weight.T
        high = turned.astype(jnp.bfloat16)
        shares[0] = high
        shares[1] = (turned - high.astype(jnp.float32)).astype(jnp.bfloat16)
        for step in range(1, ring):
            back_copy(j, source, step).wait_recv()
        tile = min(512, width)

        def body(n, carry):
            cols = pl.ds(pl.multiple_of(n * tile, tile), tile)
            rows = backbox[source, :, cols]
            store(
                cols,
                jnp.dot(shares[0], rows, preferred_element_type=jnp.float32)
                + jnp.dot(shares[1], rows, preferred_element_type=jnp.float32),
            )
            return carry

        lax.fori_loop(0, width // tile, body, 0)

    def forward_copy(source, c):
        rows = rows_of(c, piece)
        target = jnp.where(source < outer, outer + 1, outer - 1)
        return remote(
            held.at[source, rows],
            held.at[source, rows],
            hold_send.at[jnp.where(source < outer, source, source), c],
            hold_recv.at[source, c],
            target,
            mine,
        )

    def goes_on(source):
        return ((source < outer) & has_right) | ((source > outer) & has_left)

    def receive(source):
        for c in range(pieces):
            forward_copy(source, c).wait_recv()

            @pl.when(goes_on(source))
            def _():
                forward_copy(source, c).start()

    def relay_copy(dest, c):
        rows = rows_of(c, step_rows)
        leftward = dest < outer
        target = jnp.where(leftward, outer - 1, outer + 1)
        landing = jnp.where(leftward & (target == dest), count, dest)
        return remote(
            relay.at[dest, rows],
            relay.at[landing, rows],
            relay_send.at[dest, c],
            relay_recv.at[landing, c],
            target,
            mine,
        )

    def landed(place, c):
        rows = rows_of(c, step_rows)
        return remote(
            relay.at[place, rows],
            relay.at[place, rows],
            relay_send.at[0, c],
            relay_recv.at[place, c],
            lax.rem(outer + 1, count),
            mine,
        )

    def pass_on(dest):
        upstream = ((dest < outer) & has_right) | ((dest > outer) & has_left)
        for c in range(RELAYS):
            rows = rows_of(c, step_rows)

            @pl.when(upstream)
            def _():
                landed(dest, c).wait_recv()
                relay[dest, rows, :] = (
                    relay[dest, rows, :].astype(jnp.float32) + part[dest, rows, :]
                ).astype(jnp.bfloat16)

            @pl.when(jnp.logical_not(upstream))
            def _():
                relay[dest, rows, :] = part[dest, rows, :].astype(jnp.bfloat16)

            relay_copy(dest, c).start()

    order = [outer] + [lookup([arrive[m][j] for m in range(count)], outer) for j in range(count - 1)]
    drain = [lookup([leave[m][j] for m in range(count)], outer) for j in range(count - 1)]

    spread(0, outer)
    for load in loads[:3]:
        load.wait()

    def keep(cols, value):
        total[:, cols] = attended_ref[:, cols].astype(jnp.float32) + value

    feed(x_ref, length, common_gate, common_up, common_down, keep)
    for copy in info_copies:
        copy.wait_recv()

    def store_part(source):
        def store(cols, value):
            part[source, :, cols] = value

        return store

    def collect(j):
        combine(j, order[j], store_part(order[j]))
        for k in range(count - 1):
            places = [when[m][k] for m in range(count)]
            if j in places:
                if all(p == j for p in places):
                    pass_on(drain[k])
                else:

                    @pl.when(lookup([int(p == j) for p in places], outer) == 1)
                    def _():
                        pass_on(drain[k])

    last = count - 1
    between = has_left & has_right
    at_end = jnp.logical_not(between)

    def early(j):
        if j <= last:

            @pl.when(between)
            def _():
                receive(order[j])

    def late_receive(j):
        @pl.when(at_end)
        def _():
            receive(order[j])

    receive(order[1])
    spread(1, order[1])
    early(2)
    for load in loads[3:]:
        load.wait()
    serve(0, order[0], False)
    for j in range(1, last):
        if j == 1:
            serve(j, order[j], True)
        early(j + 2)
        late_receive(j + 1)
        spread(j + 1, order[j + 1])
        if j < last - 1:
            collect(j)
        if j > 1:
            serve(j, order[j], True)
    serve(last, order[last], True)
    send_back(0, order[0], range(ring))
    if last > 1:
        collect(last - 1)
    collect(last)

    def add(cols, value):
        total[:, cols] += value

    combine(0, order[0], add)
    for side, place in ((has_left, outer), (has_right, count)):
        for c in range(RELAYS):
            rows = rows_of(c, step_rows)

            @pl.when(side)
            def _():
                landed(place, c).wait_recv()
                total[rows, :] += relay[place, rows, :].astype(jnp.float32)

    out_ref[...] = total[...].astype(jnp.bfloat16)

    for copy in info_copies:
        copy.wait_send()
    for c in range(pieces):

        @pl.when(has_right)
        def _():
            own_copy(c, True).wait_send()

        @pl.when(has_left)
        def _():
            own_copy(c, False).wait_send()

    for j in range(count):
        if j > 0:
            for c in range(pieces):

                @pl.when(goes_on(order[j]))
                def _():
                    forward_copy(order[j], c).wait_send()

            for c in range(RELAYS):
                relay_copy(order[j], c).wait_send()
        for step in range(1, ring):
            go_copy(j, order[j], step).wait_send()
            back_copy(j, order[j], step).wait_send()


def outer_size(size):
    bits = size.bit_length() - 1
    return 1 << -(-bits // 3)


def experts_part(
    normed,
    attended,
    info,
    count,
    ring,
    room,
    weights,
    identity,
):
    length, width = normed.shape
    inside = weights[0].shape[1]
    shared = weights[3].shape[1]
    pieces = 2
    slots = ring * room
    bf16 = jnp.bfloat16
    vmem = pl.BlockSpec(memory_space=pltpu.VMEM)
    anywhere = pl.BlockSpec(memory_space=pl.ANY)
    dma = pltpu.SemaphoreType.DMA
    return pl.pallas_call(
        functools.partial(experts_kernel, count, ring, room, pieces),
        name="experts",
        out_shape=jax.ShapeDtypeStruct((length, width), bf16),
        in_specs=[vmem] * 3 + [anywhere] * 6,
        out_specs=vmem,
        scratch_shapes=[
            pltpu.VMEM((count, length, width), bf16),
            pltpu.VMEM((count,) + info.shape[1:], jnp.float32),
            pltpu.VMEM((count, slots, width), bf16),
            pltpu.VMEM((count, slots, width), bf16),
            pltpu.VMEM((count, slots, width), bf16),
            pltpu.VMEM((count + 1, length, width), bf16),
            pltpu.VMEM((count, length, width), jnp.float32),
            pltpu.VMEM((length, width), jnp.float32),
            pltpu.VMEM((max(slots, length), max(inside, shared)), bf16),
            pltpu.VMEM((slots, length), bf16),
            pltpu.VMEM((2, length, slots), bf16),
        ]
        + [pltpu.VMEM(w.shape, w.dtype) for w in weights]
        + [
            dma((6,)),
            dma((count,)),
            dma((count,)),
            dma((count + 1, pieces)),
            dma((count, pieces)),
            dma((count, ring)),
            dma((count, ring)),
            dma((count, ring)),
            dma((count, ring)),
            dma((count, RELAYS)),
            dma((count + 1, RELAYS)),
        ],
        compiler_params=pltpu.CompilerParams(
            collective_id=identity, has_side_effects=True, vmem_limit_bytes=67043328
        ),
    )(normed, attended, info, *weights)


def shards(
    projected_queries,
    projected_keys,
    projected_values,
    output_gate_values,
    write_strength_logits,
    decay_input_logits,
    head_rate_logarithm,
    extra_log_decay,
    per_head_norm_gain,
    output_matrix,
    residual,
    mixture_norm_gain,
    selected_expert_index,
    routing_weight,
    routed_gate_weight,
    routed_up_weight,
    routed_down_weight,
    common_gate_weight,
    common_up_weight,
    common_down_weight,
):
    heads = head_rate_logarithm.shape[0]
    count = outer_size(lax.axis_size("sp"))
    beta = jax.nn.sigmoid(write_strength_logits.astype(jnp.float32))
    decay_logarithm = extra_log_decay - jnp.exp(head_rate_logarithm)[None, :] * jax.nn.softplus(
        decay_input_logits.astype(jnp.float32) - 6.0
    )
    small = jnp.concatenate([beta, decay_logarithm], axis=1)
    small = jnp.pad(small, ((0, 0), (0, 128 - 2 * heads)))
    normed, attended = heads_part(
        projected_queries,
        projected_keys,
        projected_values,
        output_gate_values,
        small,
        per_head_norm_gain[None, :],
        residual,
        mixture_norm_gain[None, :],
        output_matrix,
        heads,
        count,
        0,
    )
    length = normed.shape[0]
    tp_size = lax.axis_size("tp")
    sp_size = lax.axis_size("sp")
    experts = sp_size * tp_size
    ring = experts // count
    room = max(2, length * TOP_K * 3 // (2 * experts))
    room = -(-room // 16) * 16
    chosen = selected_expert_index[:, :, None] == jnp.arange(experts, dtype=jnp.int32)
    named = jnp.any(chosen, axis=1)
    weight = jnp.sum(jnp.where(chosen, routing_weight[:, :, None], 0.0), axis=1)
    place = jnp.arange(length, dtype=jnp.int32)
    earlier = (place[:, None] > place[None, :]).astype(jnp.bfloat16)
    slot = jnp.dot(earlier, named.astype(jnp.bfloat16), preferred_element_type=jnp.float32)
    slot = jnp.where(named, slot, float(room))
    info = jnp.concatenate(
        [slot.T.reshape(count, ring, length), weight.T.reshape(count, ring, length)], axis=1
    )
    weights = (
        routed_gate_weight[0],
        routed_up_weight[0],
        routed_down_weight[0],
        common_gate_weight,
        common_up_weight,
        common_down_weight,
    )
    return experts_part(normed, attended, info, count, ring, room, weights, 2)


def solution(mesh):
    return jax.shard_map(
        shards,
        mesh=mesh,
        in_specs=(
            P("sp", "tp"),
            P("sp", "tp"),
            P("sp", "tp"),
            P("sp", "tp"),
            P("sp", "tp"),
            P("sp", "tp"),
            P("tp"),
            P("sp", "tp"),
            P(),
            P(),
            P(("sp", "tp"), None),
            P(),
            P(("sp", "tp"), None),
            P(("sp", "tp"), None),
            P(("sp", "tp"), None, None),
            P(("sp", "tp"), None, None),
            P(("sp", "tp"), None, None),
            P(),
            P(),
            P(),
        ),
        out_specs=P(("sp", "tp"), None),
        check_vma=False,
    )
```
